32 devices in a mesh: sp: 8 (over z, x), tp: 4 (over y, core).
Axes of the slice: x: 2, y: 2, z: 4, core: 2. Of those that a mesh axis runs over, the one named last changes fastest.
Arguments:
- resid: bfloat16 [4096, 2048], P(('sp', 'tp')), may hold values from -6 to 6
- recurrent_input: bfloat16 [4096, 2048], P('sp', 'tp'), may hold values from -12.2 to 12.2
- recurrent_out_gate: bfloat16 [4096, 2048], P('sp', 'tp'), may hold values from -6 to 6
- filter_weight: float32 [4, 2048], P(None, 'tp'), may hold values from -3 to 3
- recurrence_gate_matrix: bfloat16 [32, 64, 64], P('tp'), may hold values from -0.75 to 0.75
- input_gate_matrix: bfloat16 [32, 64, 64], P('tp'), may hold values from -0.75 to 0.75
- channel_decay_raw: float32 [2048], P('tp'), may hold values from 4.8 to 13.5
- token_decay_boost: float32 [4096, 2048], P('sp', 'tp'), may hold values from -0.7 to 0
- output_projection_weight: bfloat16 [2048, 2048], P('tp'), may hold values from -0.375 to 0.375
- expert_norm_gain: float32 [2048], replicated, may hold values from 0.1 to 1.9
- routes: int32 [4096, 2], P('sp'), may hold values from 0 to 7, all different within a row; in each aligned block of 128 rows (0 to 127, 128 to 255, ...) at most 48 rows name the same one
- expert_pair_weight: float32 [4096, 2], P(('sp', 'tp')), may hold values from 0.2 to 0.8
- gate_weight: bfloat16 [8, 2048, 2048], P('sp', None, 'tp'), may hold values from -0.125 to 0.125
- up_weight: bfloat16 [8, 2048, 2048], P('sp', None, 'tp'), may hold values from -0.125 to 0.125
- down_weight: bfloat16 [8, 2048, 2048], P('sp', None, 'tp'), may hold values from -0.25 to 0.25
Outputs:
- layer_out: bfloat16 [4096, 2048], P(('sp', 'tp'))
The draws below stay inside these ranges and needn't reach their ends.
Inputs may be any that keep to these rules, and one draw needn't show every extreme that they name: `routes`: in each aligned block of 128 rows no expert is named by more than 48 rows, and the two experts of a row differ.
All inputs are finite; a program needn't handle non-finite values.
Results may differ from the reference program's by a relative error of at most 0.013.
Values may be sent and summed in bfloat16 or wider, within the bound.
No kernel may reach another device: no remote copies, remote signals or barrier semaphores. Data moves between devices by JAX's collectives and lax.ppermute only.
A program may use at most 128 MiB of HBM per device.

```python
import math
import jax
import jax.numpy as jnp
import numpy as np
from jax import lax

D = 2048
LRU = 2048
BW = 64
HID = 2048
CONV = 4
TOK_SP = 512
BLOCKS = 32
TOKENS = 4096
ROWS_DEV = 128
EXPERTS = 8
CAP = 48
ROWS_ALL = 1536


def draw_recurrent_input(key, part):
    base_key, scale_key = jax.random.split(jax.random.fold_in(key, 11))
    base = jnp.clip(jax.random.normal(base_key, (TOKENS, LRU), jnp.float32), -6.0, 6.0)
    block_scale = jnp.exp(jax.random.uniform(scale_key, (TOKENS // TOK_SP, 1), jnp.float32, -0.7, 0.7))
    return (base * jnp.repeat(block_scale, TOK_SP, axis=0)).astype(jnp.bfloat16)


def draw_channel_decay_raw(key, part):
    pick_key, fast_key, slow_key = jax.random.split(jax.random.fold_in(key, 12), 3)
    share = 0.5
    fast = jax.random.uniform(pick_key, (LRU,), jnp.float32) < share
    quick = jax.random.uniform(fast_key, (LRU,), jnp.float32, 4.8, 6.0)
    steady = jax.random.uniform(slow_key, (LRU,), jnp.float32, 11.0, 13.5)
    return jnp.where(fast, quick, steady)


def draw_token_decay_boost(key, part):
    place_key, size_key = jax.random.split(jax.random.fold_in(key, 13))
    places = jax.random.randint(place_key, (3, LRU), 0, TOKENS)
    drops = jax.random.uniform(size_key, (3, LRU), jnp.float32, -0.7, -0.22)
    position = jnp.arange(TOKENS)[:, None]
    result = jnp.zeros((TOKENS, LRU), jnp.float32)
    for number in range(3):
        result = jnp.minimum(result, jnp.where(position == places[number][None, :], drops[number][None, :], 0.0))
    return result


def level_of(key, shape, cuts, least, high):
    loudness, own = 1.0, jax.random.fold_in(key, 6)
    for dim, blocks in cuts:
        steps = jnp.exp(jax.random.uniform(jax.random.fold_in(own, dim), (blocks,), jnp.float32, least / len(cuts), high / len(cuts)))
        loudness = loudness * jnp.repeat(steps, shape[dim] // blocks).reshape([-1 if axis == dim else 1 for axis in range(len(shape))])
    return loudness


def routed_block(own_key, own, number, rows, amount, top, limit, slope):
    ranking = jax.random.permutation(own_key, amount)
    packed, ordinary = shares(amount, rows * top, limit, slope, True), shares(amount, rows * top, limit, slope, False)
    places = jnp.arange(amount)

    def named(tallies, rotation):
        used = int((tallies > 0).sum())
        fixed = max(1, used // 4)
        shifted = fixed + (places - fixed + rotation * (used - fixed)) % max(1, amount - fixed)
        return jnp.zeros((amount,), jnp.int32).at[ranking[jnp.where(places < fixed, places, shifted)]].set(jnp.asarray(tallies, jnp.int32))

    tallies = jnp.where(number % 4 == 0, named(packed, number // 4), named(ordinary, number - number // 4 - 1))
    mixed = jax.random.permutation(jax.random.fold_in(own, 3), amount)
    donor, sink = mixed[0:amount // 2 * 2:2], mixed[1:amount // 2 * 2:2]
    margin = jnp.minimum(tallies[donor] - 1, limit - tallies[sink]) // 2
    margin = jnp.where((donor == ranking[0]) | (sink == ranking[0]) | (tallies[sink] == 0), 0, jnp.maximum(margin, 0))
    shifted = jax.random.randint(jax.random.fold_in(own, 4), (amount // 2,), 0, 1 << 20) % (margin + 1)
    tallies = tallies.at[donor].add(-shifted).at[sink].add(shifted)
    labels = jnp.searchsorted(jnp.cumsum(tallies), jnp.arange(rows * top), side="right").astype(jnp.int32)
    listing = labels.reshape(top, rows).T
    listing = listing[jax.random.permutation(jax.random.fold_in(own, 1), rows)]
    rotation = jax.random.randint(jax.random.fold_in(own, 2), (rows, 1), 0, top)
    return jnp.take_along_axis(listing, (jnp.arange(top)[None, :] + rotation) % top, axis=1)


def shares(amount, total, bound, slope, full):
    portions = [(1 << 20) // math.isqrt(standing ** slope) + 1 for standing in range(1, amount + 1)]
    largest = bound if full else min(bound, max(-(-total // amount), total * portions[0] // sum(portions)))
    least = 1 if total - largest >= amount - 1 else 0
    counts, rest = [largest] + [least] * (amount - 1), total - largest - least * (amount - 1)
    while rest > 0:
        candidates = [i for i in range(1, amount) if counts[i] < largest] or [i for i in range(1, amount) if counts[i] < bound]
        mass, remaining = sum([portions[i] for i in candidates]), rest
        for i in candidates:
            extra = min(bound - counts[i], max(1, remaining * portions[i] // mass), rest)
            counts[i] = counts[i] + extra
            rest = rest - extra
    return np.array(counts)


def normal_values(rng, extent, scale, reach, shards=(), kind=jnp.bfloat16):
    drawn = scale * jax.random.normal(rng, extent, jnp.float32)
    if shards:
        drawn = drawn * level_of(rng, extent, shards, -0.22, 0.18)
    return jnp.clip(drawn, -reach, reach).astype(kind)


def setup_inputs(seed: int = 0) -> dict:
    splits = jax.random.split(jax.random.key(seed), 16)
    resid = normal_values(splits[0], (TOKENS, D), 1.0, 6.0, ((0, 32),))
    recurrent_input = draw_recurrent_input(jax.random.fold_in(splits[15], 71), 0)
    recurrent_out_gate = normal_values(splits[2], (TOKENS, LRU), 1.0, 6.0, ((0, 8), (1, 4)))
    filter_weight = normal_values(splits[3], (CONV, LRU), 0.5, 3.0, ((1, 4),), jnp.float32)
    recurrence_gate_matrix = normal_values(splits[4], (BLOCKS, BW, BW), BW ** -0.5, 0.75, ((0, 4),))
    input_gate_matrix = normal_values(splits[5], (BLOCKS, BW, BW), BW ** -0.5, 0.75, ((0, 4),))
    channel_decay_raw = draw_channel_decay_raw(jax.random.fold_in(splits[15], 71), 0)
    token_decay_boost = draw_token_decay_boost(jax.random.fold_in(splits[15], 71), 0)
    output_projection_weight = normal_values(splits[8], (LRU, D), (LRU // 9) ** -0.5, 0.375, ((0, 4),))
    expert_norm_gain = jnp.clip(1.0 + 0.18 * jax.random.normal(splits[9], (D,), jnp.float32), 0.1, 1.9)
    routes_keys = jax.random.split(jax.random.fold_in(splits[10], 1), TOKENS // ROWS_DEV)
    routes_turns = jax.random.permutation(jax.random.fold_in(splits[10], 3), TOKENS // ROWS_DEV)
    routes = jax.vmap(lambda own, number: routed_block(jax.random.fold_in(splits[10], 2), own, number, ROWS_DEV, EXPERTS, 2, CAP, 1))(routes_keys, routes_turns).reshape((TOKENS, 2))
    expert_pair_weight = jnp.clip(0.2 + 0.6 * jax.random.uniform(splits[11], (TOKENS, 2), jnp.float32) ** level_of(splits[11], (TOKENS, 2), ((0, 32),), -0.2, 0.2), 0.2, 0.8)
    gate_weight = normal_values(splits[12], (EXPERTS, D, HID), D ** -0.5, 0.125, ((0, 8), (2, 4)))
    up_weight = normal_values(splits[13], (EXPERTS, D, HID), D ** -0.5, 0.125, ((0, 8), (2, 4)))
    down_weight = normal_values(splits[14], (EXPERTS, HID, D), (HID // 4) ** -0.5, 0.25, ((0, 8), (2, 4)))
    return dict(resid=resid, recurrent_input=recurrent_input, recurrent_out_gate=recurrent_out_gate, filter_weight=filter_weight, recurrence_gate_matrix=recurrence_gate_matrix, input_gate_matrix=input_gate_matrix, channel_decay_raw=channel_decay_raw, token_decay_boost=token_decay_boost, output_projection_weight=output_projection_weight, expert_norm_gain=expert_norm_gain, routes=routes, expert_pair_weight=expert_pair_weight, gate_weight=gate_weight, up_weight=up_weight, down_weight=down_weight)


def chain_step(earlier, later):
    return (earlier[0] * later[0], later[0] * earlier[1] + later[1])

def reference(resid, recurrent_input, recurrent_out_gate, filter_weight, recurrence_gate_matrix, input_gate_matrix, channel_decay_raw, token_decay_boost, output_projection_weight, expert_norm_gain, routes, expert_pair_weight, gate_weight, up_weight, down_weight):
    total = recurrent_input.shape[0]
    taps = filter_weight.shape[0]
    padded = jnp.pad(recurrent_input.astype(jnp.float32), ((taps - 1, 0), (0, 0)))
    mixed_in = padded[0:total] * filter_weight[0]
    for offset in range(1, taps):
        mixed_in = mixed_in + padded[offset:offset + total] * filter_weight[offset]
    smoothed = mixed_in.astype(jnp.bfloat16)
    grouped = smoothed.astype(jnp.float32).reshape(total, BLOCKS, BW)
    recurrence_gate = jax.nn.sigmoid(jnp.einsum('tni,nij->tnj', grouped, recurrence_gate_matrix.astype(jnp.float32)).reshape(total, LRU))
    input_gate = jax.nn.sigmoid(jnp.einsum('tni,nij->tnj', grouped, input_gate_matrix.astype(jnp.float32)).reshape(total, LRU))
    decay_logarithm = -8.0 * recurrence_gate * jax.nn.softplus(-channel_decay_raw) + token_decay_boost
    decay = jnp.exp(decay_logarithm)
    drive = jnp.sqrt(-jnp.expm1(2.0 * decay_logarithm)) * (input_gate * smoothed.astype(jnp.float32))
    running, state = lax.associative_scan(chain_step, (decay, drive), axis=0)
    branch = (jax.nn.gelu(recurrent_out_gate.astype(jnp.float32)) * state).astype(jnp.bfloat16)
    projected = jnp.dot(branch, output_projection_weight, preferred_element_type=jnp.float32)
    stream = (resid.astype(jnp.float32) + projected).astype(jnp.bfloat16)
    stream_wide = stream.astype(jnp.float32)
    normed = (stream_wide * lax.rsqrt(lax.optimization_barrier(jnp.mean(stream_wide * stream_wide, axis=1, keepdims=True)) + 1e-06) * expert_norm_gain).astype(jnp.bfloat16)
    flat_routes = routes.reshape(-1)
    flat_weight = expert_pair_weight.reshape(-1)
    slot_index = jnp.arange(ROWS_ALL, dtype=jnp.int32)

    def one_expert(accum, items):
        gate_part, up_part, down_part, number = items
        hits = flat_routes == number
        count = jnp.sum(hits.astype(jnp.int32))
        chosen = jnp.nonzero(hits, size=ROWS_ALL, fill_value=0)[0].astype(jnp.int32)
        valid = slot_index < count
        token = chosen // 2
        rows = normed[token]
        gate = jnp.dot(rows, gate_part, preferred_element_type=jnp.float32)
        upward = jnp.dot(rows, up_part, preferred_element_type=jnp.float32)
        active = (jax.nn.silu(gate) * upward).astype(jnp.bfloat16)
        result = jnp.dot(active, down_part, preferred_element_type=jnp.float32).astype(jnp.bfloat16).astype(jnp.float32)
        factor = jnp.where(valid, flat_weight[chosen], 0.0)
        return (accum.at[token].add(result * factor[:, None]), None)
    start = jnp.zeros((total, D), jnp.float32)
    accum, _ = lax.scan(one_expert, start, (gate_weight, up_weight, down_weight, jnp.arange(EXPERTS, dtype=jnp.int32)))
    return (stream_wide + accum).astype(jnp.bfloat16)
```

```python
import jax
import jax.numpy as jnp
from jax import lax
from jax.experimental import pallas as pl
from jax.experimental.pallas import tpu as pltpu
from jax.sharding import PartitionSpec as P

RECURRENT_SCALE = 8.0
EPSILON = 1e-06


def shifted(block, axis, distance):
    devices = range(lax.axis_size(axis))
    route = [(i - distance, i) for i in devices if i - distance in devices]
    return lax.ppermute(block, axis, route)


LANES = 128
SEGMENTS = 8


def block_diagonal(blocks):
    count, width, _ = blocks.shape
    empty = jnp.zeros((width, width), blocks.dtype)
    rows = []
    for i in range(count):
        rows.append(jnp.concatenate([blocks[i] if j == i else empty for j in range(count)], axis=1))
    return jnp.concatenate(rows, axis=0)


def scan_kernel(rim, x, taps, recur, inward, slope, boost, local, running, total, wide, decays, drives):
    tokens, lanes = x.shape
    margin = rim.shape[0]
    count = taps.shape[0]
    wide[0:margin, :] = rim[...].astype(jnp.float32)
    wide[margin : margin + tokens, :] = x[...].astype(jnp.float32)
    first = margin - count + 1
    mixed = wide[first : first + tokens, :] * taps[0:1, :]
    for j in range(1, count):
        mixed = mixed + wide[first + j : first + j + tokens, :] * taps[j : j + 1, :]
    smoothed = mixed.astype(jnp.bfloat16)
    recur_gate = jax.nn.sigmoid(
        jnp.dot(smoothed, block_diagonal(recur), preferred_element_type=jnp.float32)
    )
    input_gate = jax.nn.sigmoid(
        jnp.dot(smoothed, block_diagonal(inward), preferred_element_type=jnp.float32)
    )
    log_decay = -RECURRENT_SCALE * recur_gate * slope[...] + boost[...]
    decay = jnp.exp(log_decay)
    twice = 2.0 * log_decay
    series = 1.0 + twice * (1.0 / 9.0)
    for n in range(8, 1, -1):
        series = 1.0 + twice * (1.0 / n) * series
    lost = jnp.where(twice > -0.35, -twice * series, 1.0 - decay * decay)
    decays[...] = decay
    drives[...] = jnp.sqrt(lost) * (input_gate * smoothed.astype(jnp.float32))
    length = tokens // SEGMENTS

    def step(j, held):
        product, state = held
        here = pl.ds(j, SEGMENTS, stride=length)
        a = decays[here, :]
        state = a * state + drives[here, :]
        product = product * a
        local[here, :] = state
        running[here, :] = product
        return product, state

    product, state = lax.fori_loop(
        0,
        length,
        step,
        (jnp.ones((SEGMENTS, lanes), jnp.float32), jnp.zeros((SEGMENTS, lanes), jnp.float32)),
        unroll=8,
    )
    a, b = product[0:1], state[0:1]
    for k in range(1, SEGMENTS):
        a, b = a * product[k : k + 1], product[k : k + 1] * b + state[k : k + 1]
    total[0:1, :] = a
    total[1:2, :] = b


def local_scan(rim, x, taps, recur, inward, slope, boost):
    tokens, channels = x.shape
    lanes = min(LANES, channels)
    width = recur.shape[1]
    column = lambda rows: pl.BlockSpec((rows, lanes), lambda i: (0, i))
    blocks = pl.BlockSpec((lanes // width, width, width), lambda i: (i, 0, 0))
    wide = jax.ShapeDtypeStruct((tokens, channels), jnp.float32)
    return pl.pallas_call(
        scan_kernel,
        grid=(channels // lanes,),
        in_specs=[
            column(rim.shape[0]),
            column(tokens),
            column(taps.shape[0]),
            blocks,
            blocks,
            column(1),
            column(tokens),
        ],
        out_specs=[column(tokens), column(tokens), column(2)],
        out_shape=[wide, wide, jax.ShapeDtypeStruct((2, channels), jnp.float32)],
        scratch_shapes=[
            pltpu.VMEM((tokens + rim.shape[0], lanes), jnp.float32),
            pltpu.VMEM((tokens, lanes), jnp.float32),
            pltpu.VMEM((tokens, lanes), jnp.float32),
        ],
        name="local_scan",
    )(rim, x, taps, recur, inward, slope, boost)


def branch_kernel(position, totals, local, running, gate, branch):
    tokens, lanes = local.shape
    entering = jnp.zeros((1, lanes), jnp.float32)
    for k in range(totals.shape[0]):
        passed = totals[k, 0:1, :] * entering + totals[k, 1:2, :]
        entering = jnp.where(k < position[0], passed, entering)
    length = tokens // SEGMENTS
    for k in range(SEGMENTS):
        here = slice(k * length, (k + 1) * length)
        state = local[here, :] + running[here, :] * entering
        opened = jax.nn.gelu(gate[here, :].astype(jnp.float32))
        branch[here, :] = (opened * state).astype(jnp.bfloat16)
        entering = state[length - 1 : length]


def finish_branch(position, totals, local, running, gate):
    tokens, channels = local.shape
    lanes = min(LANES, channels)
    column = lambda rows: pl.BlockSpec((rows, lanes), lambda i: (0, i))
    return pl.pallas_call(
        branch_kernel,
        grid=(channels // lanes,),
        in_specs=[
            pl.BlockSpec(memory_space=pltpu.SMEM),
            pl.BlockSpec((totals.shape[0], 2, lanes), lambda i: (0, 0, i)),
            column(tokens),
            column(tokens),
            column(tokens),
        ],
        out_specs=column(tokens),
        out_shape=jax.ShapeDtypeStruct((tokens, channels), jnp.bfloat16),
        name="finish_branch",
    )(position, totals, local, running, gate)


def slot_numbers(picks, experts):
    flat = picks.reshape(-1)
    onehot = (flat[:, None] == jnp.arange(experts, dtype=jnp.int32)[None, :]).astype(jnp.int32)
    before = jnp.cumsum(onehot, axis=0) - onehot
    return (flat, jnp.sum(before * onehot, axis=1))


def fill_slots(source_rows, slot_of, row_of, slot_count):
    match = slot_of[None, :] == jnp.arange(slot_count, dtype=jnp.int32)[:, None]
    picked = jnp.sum(jnp.where(match, row_of[None, :], 0), axis=1)
    present = jnp.any(match, axis=1)
    return jnp.where(present[:, None], source_rows[picked], jnp.zeros((), source_rows.dtype))


def expert_hidden(rows, gate_weight, up_weight):
    gate = jnp.dot(rows, gate_weight[0], preferred_element_type=jnp.float32)
    upward = jnp.dot(rows, up_weight[0], preferred_element_type=jnp.float32)
    return (jax.nn.silu(gate) * upward).astype(jnp.bfloat16)


def expert_down(active, down_weight):
    columns = down_weight[0]
    return jnp.dot(
        lax.all_gather(active, "tp", axis=1, tiled=True),
        columns,
        preferred_element_type=jnp.float32,
    ).astype(jnp.bfloat16)


def body(
    resid,
    recurrent_input,
    recurrent_out_gate,
    filter_weight,
    recurrence_gate_matrix,
    input_gate_matrix,
    channel_decay_raw,
    token_decay_boost,
    output_projection_weight,
    expert_norm_gain,
    routes,
    expert_pair_weight,
    gate_weight,
    up_weight,
    down_weight,
):
    tokens_here, channels = recurrent_input.shape
    rim = shifted(recurrent_input[tokens_here - 8 :], "sp", 1)
    slope = jax.nn.softplus(-channel_decay_raw)[None, :]
    local, running, total = local_scan(
        rim,
        recurrent_input,
        filter_weight,
        recurrence_gate_matrix,
        input_gate_matrix,
        slope,
        token_decay_boost,
    )
    totals = lax.all_gather(total, "sp")
    position = lax.axis_index("sp").astype(jnp.int32).reshape(1)
    branch = finish_branch(position, totals, local, running, recurrent_out_gate)
    tp_size = lax.axis_size("tp")
    rows_dev = tokens_here // tp_size
    projected = lax.psum_scatter(
        jnp.dot(branch, output_projection_weight, preferred_element_type=jnp.float32),
        "tp",
        scatter_dimension=0,
        tiled=True,
    )
    stream = (resid.astype(jnp.float32) + projected).astype(jnp.bfloat16)
    stream_wide = stream.astype(jnp.float32)
    normed = (
        stream_wide
        * lax.rsqrt(jnp.mean(stream_wide * stream_wide, axis=1, keepdims=True) + EPSILON)
        * expert_norm_gain
    ).astype(jnp.bfloat16)
    model_width = normed.shape[1]
    experts = lax.axis_size("sp")
    capacity = max(2, 3 * rows_dev // experts)
    own_routes = lax.dynamic_slice_in_dim(routes, lax.axis_index("tp") * rows_dev, rows_dev, 0)
    own_flat, own_rank = slot_numbers(own_routes, experts)
    own_slots = own_flat * capacity + own_rank
    row_of = jnp.arange(2 * rows_dev, dtype=jnp.int32) // 2
    outgoing = fill_slots(normed, own_slots, row_of, experts * capacity).reshape(
        experts, capacity, model_width
    )
    arrived = lax.all_to_all(outgoing, "sp", split_axis=0, concat_axis=0, tiled=True)
    piece = lax.all_gather(
        arrived.reshape(1, experts * capacity, model_width), "tp", axis=0, tiled=True
    )
    flat_rows = piece.reshape(piece.shape[0] * piece.shape[1], model_width)
    active = expert_hidden(flat_rows, gate_weight, up_weight).reshape(
        piece.shape[0], piece.shape[1], -1
    )
    result = expert_down(active.reshape(-1, active.shape[2]), down_weight)
    joined = lax.all_to_all(
        result.reshape(tp_size, experts * capacity, -1),
        "tp",
        split_axis=0,
        concat_axis=2,
        tiled=True,
    )
    returned = lax.all_to_all(
        joined.reshape(experts, capacity, model_width),
        "sp",
        split_axis=0,
        concat_axis=0,
        tiled=True,
    )
    picked = (
        returned.reshape(experts * capacity, model_width)[own_slots]
        .astype(jnp.float32)
        .reshape(rows_dev, 2, model_width)
    )
    blended = jnp.sum(picked * expert_pair_weight[:, :, None], axis=1)
    return (stream_wide + blended).astype(jnp.bfloat16)


def solution(mesh):
    placed = (
        P(("sp", "tp"), None),
        P("sp", "tp"),
        P("sp", "tp"),
        P(None, "tp"),
        P("tp", None, None),
        P("tp", None, None),
        P("tp"),
        P("sp", "tp"),
        P("tp", None),
        P(),
        P("sp", None),
        P(("sp", "tp"), None),
        P("sp", None, "tp"),
        P("sp", None, "tp"),
        P("sp", None, "tp"),
    )
    return jax.shard_map(
        body, mesh=mesh, in_specs=placed, out_specs=P(("sp", "tp"), None), check_vma=False
    )
```

```python
import functools

import jax
import jax.numpy as jnp
from jax import lax
from jax.experimental import pallas as pl
from jax.experimental.pallas import tpu as pltpu
from jax.sharding import PartitionSpec as P

RECURRENT_SCALE = 8.0
EPSILON = 1e-06


def shifted(block, axis, distance):
    devices = range(lax.axis_size(axis))
    route = [(i - distance, i) for i in devices if i - distance in devices]
    return lax.ppermute(block, axis, route)


def across(block, bits):
    return lax.ppermute(block, "sp", [(i, i ^ bits) for i in range(lax.axis_size("sp"))])


def swapped(block):
    return lax.ppermute(block, "tp", [(i, i ^ 1) for i in range(lax.axis_size("tp"))])


def turned(block, distance):
    size = lax.axis_size("tp")
    return lax.ppermute(block, "tp", [(i, (i + 2 * distance) % size) for i in range(size)])


LANES = 128
SEGMENTS = 8


def block_diagonal(blocks):
    count, width, _ = blocks.shape
    empty = jnp.zeros((width, width), blocks.dtype)
    rows = []
    for i in range(count):
        rows.append(jnp.concatenate([blocks[i] if j == i else empty for j in range(count)], axis=1))
    return jnp.concatenate(rows, axis=0)


def scan_kernel(rim, x, taps, recur, inward, slope, boost, local, running, total, wide, decays, drives):
    tokens, lanes = x.shape
    margin = rim.shape[0]
    count = taps.shape[0]
    wide[0:margin, :] = rim[...].astype(jnp.float32)
    wide[margin : margin + tokens, :] = x[...].astype(jnp.float32)
    first = margin - count + 1
    mixed = wide[first : first + tokens, :] * taps[0:1, :]
    for j in range(1, count):
        mixed = mixed + wide[first + j : first + j + tokens, :] * taps[j : j + 1, :]
    smoothed = mixed.astype(jnp.bfloat16)
    recur_gate = jax.nn.sigmoid(
        jnp.dot(smoothed, block_diagonal(recur), preferred_element_type=jnp.float32)
    )
    input_gate = jax.nn.sigmoid(
        jnp.dot(smoothed, block_diagonal(inward), preferred_element_type=jnp.float32)
    )
    log_decay = -RECURRENT_SCALE * recur_gate * slope[...] + boost[...]
    decay = jnp.exp(log_decay)
    twice = 2.0 * log_decay
    series = 1.0 + twice * (1.0 / 9.0)
    for n in range(8, 1, -1):
        series = 1.0 + twice * (1.0 / n) * series
    lost = jnp.where(twice > -0.35, -twice * series, 1.0 - decay * decay)
    decays[...] = decay
    drives[...] = jnp.sqrt(lost) * (input_gate * smoothed.astype(jnp.float32))
    length = tokens // SEGMENTS

    def step(j, held):
        product, state = held
        here = pl.ds(j, SEGMENTS, stride=length)
        a = decays[here, :]
        state = a * state + drives[here, :]
        product = product * a
        local[here, :] = state
        running[here, :] = product
        return product, state

    product, state = lax.fori_loop(
        0,
        length,
        step,
        (jnp.ones((SEGMENTS, lanes), jnp.float32), jnp.zeros((SEGMENTS, lanes), jnp.float32)),
        unroll=8,
    )
    a, b = product[0:1], state[0:1]
    for k in range(1, SEGMENTS):
        a, b = a * product[k : k + 1], product[k : k + 1] * b + state[k : k + 1]
    total[0:1, :] = a
    total[1:2, :] = b


def local_scan(rim, x, taps, recur, inward, slope, boost):
    tokens, channels = x.shape
    lanes = min(LANES, channels)
    width = recur.shape[1]
    column = lambda rows: pl.BlockSpec((rows, lanes), lambda i: (0, i))
    blocks = pl.BlockSpec((lanes // width, width, width), lambda i: (i, 0, 0))
    wide = jax.ShapeDtypeStruct((tokens, channels), jnp.float32)
    return pl.pallas_call(
        scan_kernel,
        grid=(channels // lanes,),
        in_specs=[
            column(rim.shape[0]),
            column(tokens),
            column(taps.shape[0]),
            blocks,
            blocks,
            column(1),
            column(tokens),
        ],
        out_specs=[column(tokens), column(tokens), column(2)],
        out_shape=[wide, wide, jax.ShapeDtypeStruct((2, channels), jnp.float32)],
        scratch_shapes=[
            pltpu.VMEM((tokens + rim.shape[0], lanes), jnp.float32),
            pltpu.VMEM((tokens, lanes), jnp.float32),
            pltpu.VMEM((tokens, lanes), jnp.float32),
        ],
        name="local_scan",
    )(rim, x, taps, recur, inward, slope, boost)


def branch_kernel(place, entering, local, running, gate, keep, give):
    tokens, lanes = local.shape
    length = tokens // SEGMENTS
    pairs, rows = keep.shape[0], keep.shape[1]
    step = min(length, rows)
    begin = entering[...]
    for start in range(0, tokens, step):
        here = slice(start, start + step)
        state = local[here, :] + running[here, :] * begin
        opened = jax.nn.gelu(gate[here, :].astype(jnp.float32))
        value = (opened * state).astype(jnp.bfloat16)
        block = start // rows
        slot = lax.rem(block // 2 - place[0] + pairs, pairs)
        inside = slice(start % rows, start % rows + step)
        mine = place[1] == block % 2

        @pl.when(mine)
        def _():
            keep[slot, inside, :] = value

        @pl.when(jnp.logical_not(mine))
        def _():
            give[slot, inside, :] = value

        if (start + step) % length == 0:
            begin = state[step - 1 : step]


def finish_branch(place, entering, local, running, gate, pairs):
    tokens, channels = local.shape
    lanes = min(LANES, channels)
    column = lambda rows: pl.BlockSpec((rows, lanes), lambda i: (0, i))
    rows = tokens // (2 * pairs)
    half = jax.ShapeDtypeStruct((pairs, rows, channels), jnp.bfloat16)
    return pl.pallas_call(
        branch_kernel,
        grid=(channels // lanes,),
        in_specs=[
            pl.BlockSpec(memory_space=pltpu.SMEM),
            column(1),
            column(tokens),
            column(tokens),
            column(tokens),
        ],
        out_specs=[pl.BlockSpec((pairs, rows, lanes), lambda i: (0, 0, i))] * 2,
        out_shape=[half, half],
        cost_estimate=pl.CostEstimate(
            flops=20 * tokens * channels, bytes_accessed=12 * tokens * channels, transcendentals=0
        ),
        name="finish_branch",
    )(place, entering, local, running, gate)


def padded(count):
    return -(-count // 16) * 16


def send_kernel(resid, own, gain, slots, *refs, experts):
    pieces, (stream, *blocks) = refs[: -1 - experts], refs[-1 - experts :]
    total = own[...]
    for piece in pieces:
        total = total + piece[...].astype(jnp.float32)
    rounded = (resid[...].astype(jnp.float32) + total).astype(jnp.bfloat16)
    stream[...] = rounded
    wide = rounded.astype(jnp.float32)
    scale = lax.rsqrt(jnp.mean(wide * wide, axis=1, keepdims=True) + EPSILON)
    normed = (wide * scale * gain[...]).astype(jnp.bfloat16)
    rows = resid.shape[0]
    stride = padded(blocks[0].shape[0])
    numbers = lax.broadcasted_iota(jnp.int32, (len(blocks) * stride, rows), 0)
    hit = (numbers == slots[0:1, :]) | (numbers == slots[1:2, :])
    picked = jnp.dot(
        hit.astype(jnp.float32).astype(jnp.bfloat16), normed, preferred_element_type=jnp.float32
    ).astype(jnp.bfloat16)
    for i, block in enumerate(blocks):
        block[...] = picked[i * stride : i * stride + block.shape[0]]


def send_rows(resid, own, pieces, gain, slots, experts, capacity):
    rows, width = resid.shape
    block = jax.ShapeDtypeStruct((capacity, width), jnp.bfloat16)
    stream, *blocks = pl.pallas_call(
        functools.partial(send_kernel, experts=experts),
        out_shape=[jax.ShapeDtypeStruct((rows, width), jnp.bfloat16)] + [block] * experts,
        cost_estimate=pl.CostEstimate(
            flops=2 * rows * width * experts * capacity,
            bytes_accessed=8 * rows * width,
            transcendentals=0,
        ),
        name="send_rows",
    )(resid, own, gain, slots, *pieces)
    return stream, blocks


def expert_kernel(place, *refs, counts):
    groups, pairs, near_blocks = counts
    rows_in, refs = refs[:groups], refs[groups:]
    gate_own, gate_far, up_own, up_far = refs[:4]
    down_own, down_far = refs[4 : 4 + pairs], refs[4 + pairs : 4 + 2 * pairs]
    rows_out = refs[4 + 2 * pairs : 4 + 2 * pairs + groups]
    left, total = refs[4 + 2 * pairs + groups :]
    step = pl.program_id(0)

    @pl.when(step == 0)
    def _():
        at = 0
        for block in rows_in:
            left[at : at + block.shape[0], :] = block[...]
            at += padded(block.shape[0])
        total[...] = jnp.zeros(total.shape, total.dtype)

    def part(gate_block, up_block):
        gate = jnp.dot(left[...], gate_block[...], preferred_element_type=jnp.float32)
        upward = jnp.dot(left[...], up_block[...], preferred_element_type=jnp.float32)
        active = (jax.nn.silu(gate) * upward).astype(jnp.bfloat16)
        for side, pieces in enumerate((down_own, down_far)):
            core = place[1] if side == 0 else 1 - place[1]
            for d, piece in enumerate(pieces):
                width = piece.shape[1]
                column = (lax.rem(place[0] - d + pairs, pairs) * 2 + core) * width
                here = pl.ds(pl.multiple_of(column, width), width)
                total[:, here] += jnp.dot(active, piece[...], preferred_element_type=jnp.float32)

    @pl.when(step < near_blocks)
    def _():
        part(gate_own, up_own)

    @pl.when(step >= near_blocks)
    def _():
        part(gate_far, up_far)

    @pl.when(step == pl.num_programs(0) - 1)
    def _():
        at = 0
        for block in rows_out:
            block[...] = total[at : at + block.shape[0], :].astype(block.dtype)
            at += padded(block.shape[0])


def expert_rows(place, rows, weights, kind):
    gate_own, gate_far, up_own, up_far, down_own, down_far = weights
    model, hidden = gate_own.shape
    pairs = len(down_own)
    step = min(256, hidden)
    near = hidden // step
    width = down_own[0].shape[1]
    whole = lambda a: pl.BlockSpec(a.shape, lambda j, p: (0, 0))
    own = pl.BlockSpec((model, step), lambda j, p: (0, jnp.minimum(j, near - 1)))
    far = pl.BlockSpec((model, step), lambda j, p: (0, jnp.maximum(j - near, 0)))
    down = pl.BlockSpec(
        (step, width),
        lambda j, p: (jnp.where(j < near, p[1] * near + j, (1 - p[1]) * near + j - near), 0),
    )
    height = sum(padded(a.shape[0]) for a in rows)
    return pl.pallas_call(
        functools.partial(expert_kernel, counts=(len(rows), pairs, near)),
        grid_spec=pltpu.PrefetchScalarGridSpec(
            num_scalar_prefetch=1,
            grid=(2 * near,),
            in_specs=[whole(a) for a in rows] + [own, far, own, far] + [down] * (2 * pairs),
            out_specs=[whole(a) for a in rows],
            scratch_shapes=[
                pltpu.VMEM((height, model), jnp.bfloat16),
                pltpu.VMEM((height, model), jnp.float32),
            ],
        ),
        out_shape=[jax.ShapeDtypeStruct(a.shape, kind) for a in rows],
        cost_estimate=pl.CostEstimate(
            flops=12 * height * model * hidden,
            bytes_accessed=12 * model * hidden,
            transcendentals=0,
        ),
        name="expert_rows",
    )(place, *rows, gate_own, gate_far, up_own, up_far, *down_own, *down_far)


def blend_kernel(stream, slots, pair_weight, *refs):
    blocks, (out, table) = refs[:-2], refs[-2:]
    rows = stream.shape[0]
    stride = padded(blocks[0].shape[0])
    if stride != blocks[0].shape[0]:
        table[...] = jnp.zeros(table.shape, table.dtype)
    for i, block in enumerate(blocks):
        table[i * stride : i * stride + block.shape[0], :] = block[...]
    numbers = lax.broadcasted_iota(jnp.int32, (rows, table.shape[0]), 1)
    mix = jnp.where(numbers == slots[:, 0:1], pair_weight[:, 0:1], 0.0)
    mix = mix + jnp.where(numbers == slots[:, 1:2], pair_weight[:, 1:2], 0.0)
    high = mix.astype(jnp.bfloat16)
    low = (mix - high.astype(jnp.float32)).astype(jnp.bfloat16)
    rows_back = table[...]
    blended = jnp.dot(high, rows_back, preferred_element_type=jnp.float32)
    blended = blended + jnp.dot(low, rows_back, preferred_element_type=jnp.float32)
    out[...] = (stream[...].astype(jnp.float32) + blended).astype(jnp.bfloat16)


def blend_rows(stream, slots, pair_weight, blocks):
    rows, width = stream.shape
    lanes = min(512, width)
    column = lambda count: pl.BlockSpec((count, lanes), lambda i: (0, i))
    fixed = lambda a: pl.BlockSpec(a.shape, lambda i: (0, 0))
    height = len(blocks) * padded(blocks[0].shape[0])
    return pl.pallas_call(
        blend_kernel,
        grid=(width // lanes,),
        in_specs=[column(rows), fixed(slots), fixed(pair_weight)]
        + [column(b.shape[0]) for b in blocks],
        out_specs=column(rows),
        out_shape=jax.ShapeDtypeStruct((rows, width), jnp.bfloat16),
        scratch_shapes=[pltpu.VMEM((height, lanes), jnp.bfloat16)],
        cost_estimate=pl.CostEstimate(
            flops=4 * rows * width * height, bytes_accessed=10 * rows * width, transcendentals=0
        ),
        name="blend_rows",
    )(stream, slots, pair_weight, *blocks)


def slot_numbers(picks, experts):
    flat = picks.reshape(-1)
    onehot = (flat[:, None] == jnp.arange(experts, dtype=jnp.int32)[None, :]).astype(jnp.int32)
    before = jnp.cumsum(onehot, axis=0) - onehot
    return (flat, jnp.sum(before * onehot, axis=1))


def entering_state(total, me):
    size = lax.axis_size("sp")
    a, b = total[0:1], total[1:2]
    before = jnp.zeros_like(b)
    passed = jnp.ones_like(a)
    bit = 1
    while bit < size:
        other = across(jnp.concatenate([a, b], axis=0), bit)
        oa, ob = other[0:1], other[1:2]
        after = (me & bit) != 0
        before = jnp.where(after, passed * ob + before, before)
        passed = jnp.where(after, passed * oa, passed)
        b = jnp.where(after, a * ob + b, oa * b + ob)
        a = a * oa
        bit *= 2
    return before


def body(
    resid,
    recurrent_input,
    recurrent_out_gate,
    filter_weight,
    recurrence_gate_matrix,
    input_gate_matrix,
    channel_decay_raw,
    token_decay_boost,
    output_projection_weight,
    expert_norm_gain,
    routes,
    expert_pair_weight,
    gate_weight,
    up_weight,
    down_weight,
):
    tokens_here = recurrent_input.shape[0]
    tp_size, experts = lax.axis_size("tp"), lax.axis_size("sp")
    me, column = lax.axis_index("sp"), lax.axis_index("tp")
    pairs = tp_size // 2
    row, core = column // 2, column % 2
    place = jnp.stack([row, core]).astype(jnp.int32)
    rows_dev = tokens_here // tp_size
    capacity = max(2, 3 * rows_dev // experts)

    rim = shifted(recurrent_input[tokens_here - 8 :], "sp", 1)
    slope = jax.nn.softplus(-channel_decay_raw)[None, :]
    local, running, total = local_scan(
        rim,
        recurrent_input,
        filter_weight,
        recurrence_gate_matrix,
        input_gate_matrix,
        slope,
        token_decay_boost,
    )

    total, gate_own, up_own, down_all = lax.optimization_barrier(
        (total, gate_weight[0], up_weight[0], down_weight[0])
    )
    projection_far = swapped(output_projection_weight)
    strip = down_all.shape[0] // pairs
    strip_of = lambda d: lax.dynamic_slice_in_dim(down_all, lax.rem(row + d, pairs) * strip, strip, 0)
    down_own = [strip_of(0)] + [turned(strip_of(d), d) for d in range(1, pairs)]
    gate_far, up_far = swapped(gate_own), swapped(up_own)
    down_far = [swapped(piece) for piece in down_own]
    weights = (gate_own, gate_far, up_own, up_far, down_own, down_far)

    own_routes = lax.dynamic_slice_in_dim(routes, column * rows_dev, rows_dev, 0)
    own_flat, own_rank = slot_numbers(own_routes, experts)
    slots = ((own_flat ^ me) * padded(capacity) + own_rank).reshape(rows_dev, 2)

    before = entering_state(total, me)
    keep, give = finish_branch(place, before, local, running, recurrent_out_gate, pairs)
    taken = swapped(give)

    def projected(d):
        near = jnp.dot(keep[d], output_projection_weight, preferred_element_type=jnp.float32)
        return near + jnp.dot(taken[d], projection_far, preferred_element_type=jnp.float32)

    pieces = [turned(projected(d).astype(jnp.bfloat16), d) for d in range(1, pairs)]
    stream, blocks = send_rows(
        resid,
        projected(0),
        pieces,
        expert_norm_gain[None, :],
        slots.T,
        experts,
        capacity,
    )
    quarter = experts // 4
    cuts = [(0, 1), (1, 2 * quarter), (2 * quarter, 3 * quarter), (3 * quarter, experts)]
    order = list(range(2 * quarter, experts)) + list(range(1, 2 * quarter))
    arrived = {0: blocks[0]}
    for k in order:
        arrived[k] = across(blocks[k], k)
    own_rows = [jnp.concatenate([arrived[k] for k in range(*cut)], axis=0) for cut in cuts]
    their_rows = [[turned(g, d) for g in own_rows] for d in range(1, pairs)]
    own_parts = expert_rows(place, own_rows, weights, jnp.float32)
    their_parts = expert_rows(place, [g for rows in their_rows for g in rows], weights, jnp.bfloat16)
    returned = {}
    for i in (2, 3, 1, 0):
        wide = own_parts[i]
        for d in range(1, pairs):
            wide = wide + turned(their_parts[(d - 1) * len(cuts) + i], pairs - d).astype(jnp.float32)
        first = cuts[i][0]
        for k in range(*cuts[i]):
            result = wide[(k - first) * capacity : (k - first + 1) * capacity].astype(jnp.bfloat16)
            returned[k] = across(result, k) if k else result
    return blend_rows(stream, slots, expert_pair_weight, [returned[k] for k in range(experts)])


def solution(mesh):
    placed = (
        P(("sp", "tp"), None),
        P("sp", "tp"),
        P("sp", "tp"),
        P(None, "tp"),
        P("tp", None, None),
        P("tp", None, None),
        P("tp"),
        P("sp", "tp"),
        P("tp", None),
        P(),
        P("sp", None),
        P(("sp", "tp"), None),
        P("sp", None, "tp"),
        P("sp", None, "tp"),
        P("sp", None, "tp"),
    )
    return jax.shard_map(
        body, mesh=mesh, in_specs=placed, out_specs=P(("sp", "tp"), None), check_vma=False
    )
```

```python
import functools

import jax
import jax.numpy as jnp
from jax import lax
from jax.experimental import pallas as pl
from jax.experimental.pallas import tpu as pltpu
from jax.sharding import PartitionSpec as P


RECURRENT_SCALE = 8.0
EPSILON = 1e-06


def granted(mebibytes):
    return pltpu.CompilerParams(vmem_limit_bytes=mebibytes * 2**20)


def shifted(block):
    size = lax.axis_size("sp")
    return lax.ppermute(block, "sp", [(i, i + 1) for i in range(size - 1)])


def across(block, bits):
    return lax.ppermute(block, "sp", [(i, i ^ bits) for i in range(lax.axis_size("sp"))])


def swapped(block):
    return lax.ppermute(block, "tp", [(i, i ^ 1) for i in range(lax.axis_size("tp"))])


def turned(block, distance):
    size = lax.axis_size("tp")
    return lax.ppermute(block, "tp", [(i, (i + 2 * distance) % size) for i in range(size)])


LANES = 128
GROUPS = 2
SEGMENTS = 8


def block_diagonal(blocks):
    count, width, _ = blocks.shape
    empty = jnp.zeros((width, width), blocks.dtype)
    rows = []
    for i in range(count):
        rows.append(jnp.concatenate([blocks[i] if j == i else empty for j in range(count)], axis=1))
    return jnp.concatenate(rows, axis=0)


def scan_kernel(rim, x, taps, recur, inward, slope, boost, local, running, total, wide, decays, drives):
    tokens, _ = x.shape
    margin = rim.shape[0]
    count = taps.shape[0]
    wide[0:margin, :] = rim[...].astype(jnp.float32)
    wide[margin : margin + tokens, :] = x[...].astype(jnp.float32)
    first = margin - count + 1
    mixed = wide[first : first + tokens, :] * taps[0:1, :]
    for j in range(1, count):
        mixed = mixed + wide[first + j : first + j + tokens, :] * taps[j : j + 1, :]
    smoothed = mixed.astype(jnp.bfloat16)
    recur_gate = jax.nn.sigmoid(
        jnp.dot(smoothed, block_diagonal(recur), preferred_element_type=jnp.float32)
    )
    input_gate = jax.nn.sigmoid(
        jnp.dot(smoothed, block_diagonal(inward), preferred_element_type=jnp.float32)
    )
    log_decay = -RECURRENT_SCALE * recur_gate * jax.nn.softplus(-slope[...]) + boost[...]
    decay = jnp.exp(log_decay)
    twice = 2.0 * log_decay
    series = 1.0 + twice * (1.0 / 9.0)
    for n in range(8, 1, -1):
        series = 1.0 + twice * (1.0 / n) * series
    lost = jnp.where(twice > -0.35, -twice * series, 1.0 - decay * decay)
    drive = jnp.sqrt(lost) * (input_gate * smoothed.astype(jnp.float32))
    groups, width = decays.shape[0], decays.shape[2]
    for g in range(groups):
        decays[g] = decay[:, g * width : (g + 1) * width]
        drives[g] = drive[:, g * width : (g + 1) * width]
    length = tokens // SEGMENTS

    def step(j, held):
        here = pl.ds(j, SEGMENTS, stride=length)
        after = []
        for g, (product, state) in enumerate(held):
            a = decays[g, here, :]
            state = a * state + drives[g, here, :]
            product = product * a
            local[g, here, :] = state
            running[g, here, :] = product
            after.append((product, state))
        return tuple(after)

    start = (jnp.ones((SEGMENTS, width), jnp.float32), jnp.zeros((SEGMENTS, width), jnp.float32))
    ends = lax.fori_loop(0, length, step, (start,) * groups, unroll=8)
    for g, (product, state) in enumerate(ends):
        a, b = product[0:1], state[0:1]
        for k in range(1, SEGMENTS):
            a, b = a * product[k : k + 1], product[k : k + 1] * b + state[k : k + 1]
        total[0:1, g * width : (g + 1) * width] = a
        total[1:2, g * width : (g + 1) * width] = b


def local_scan(rim, x, taps, recur, inward, slope, boost):
    tokens, channels = x.shape
    groups = min(GROUPS, channels // LANES)
    lanes = groups * LANES
    width = recur.shape[1]
    folded = pl.BlockSpec((groups, tokens, LANES), lambda i: (i, 0, 0))
    column = lambda rows: pl.BlockSpec((rows, lanes), lambda i: (0, i))
    blocks = pl.BlockSpec((lanes // width, width, width), lambda i: (i, 0, 0))
    wide = jax.ShapeDtypeStruct((channels // LANES, tokens, LANES), jnp.float32)
    return pl.pallas_call(
        scan_kernel,
        grid=(channels // lanes,),
        in_specs=[
            column(rim.shape[0]),
            column(tokens),
            column(taps.shape[0]),
            blocks,
            blocks,
            column(1),
            column(tokens),
        ],
        out_specs=[folded, folded, column(2)],
        out_shape=[wide, wide, jax.ShapeDtypeStruct((2, channels), jnp.float32)],
        scratch_shapes=[
            pltpu.VMEM((tokens + rim.shape[0], lanes), jnp.float32),
            pltpu.VMEM((groups, tokens, LANES), jnp.float32),
            pltpu.VMEM((groups, tokens, LANES), jnp.float32),
        ],
        name="local_scan",
    )(rim, x, taps, recur, inward, slope, boost)


def branch_kernel(place, entering, local, running, gate, keep, give):
    groups, tokens, width = local.shape
    length = tokens // SEGMENTS
    pairs, rows = keep.shape[0], keep.shape[1]
    step = min(length, rows)
    begins = [entering[:, g * width : (g + 1) * width] for g in range(groups)]
    for start in range(0, tokens, step):
        here = slice(start, start + step)
        states = [local[g, here, :] + running[g, here, :] * begins[g] for g in range(groups)]
        opened = jax.nn.gelu(gate[here, :].astype(jnp.float32))
        value = (opened * jnp.concatenate(states, axis=1)).astype(jnp.bfloat16)
        block = start // rows
        slot = lax.rem(block // 2 - place[0] + pairs, pairs)
        inside = slice(start % rows, start % rows + step)
        mine = place[1] == block % 2

        @pl.when(mine)
        def _():
            keep[slot, inside, :] = value

        @pl.when(jnp.logical_not(mine))
        def _():
            give[slot, inside, :] = value

        if (start + step) % length == 0:
            begins = [state[step - 1 : step] for state in states]


def finish_branch(place, entering, local, running, gate, pairs):
    tokens, channels = gate.shape
    groups = min(GROUPS, channels // LANES)
    lanes = groups * LANES
    column = lambda rows: pl.BlockSpec((rows, lanes), lambda i: (0, i))
    folded = pl.BlockSpec((groups, tokens, LANES), lambda i: (i, 0, 0))
    rows = tokens // (2 * pairs)
    half = jax.ShapeDtypeStruct((pairs, rows, channels), jnp.bfloat16)
    return pl.pallas_call(
        branch_kernel,
        grid=(channels // lanes,),
        in_specs=[
            pl.BlockSpec(memory_space=pltpu.SMEM),
            column(1),
            folded,
            folded,
            column(tokens),
        ],
        out_specs=[pl.BlockSpec((pairs, rows, lanes), lambda i: (0, 0, i))] * 2,
        out_shape=[half, half],
        cost_estimate=pl.CostEstimate(
            flops=20 * tokens * channels, bytes_accessed=12 * tokens * channels, transcendentals=0
        ),
        name="finish_branch",
    )(place, entering, local, running, gate)


def padded(count):
    return -(-count // 16) * 16


def send_kernel(resid, own, gain, slots, *refs, experts):
    pieces, (stream, *blocks) = refs[: -1 - experts], refs[-1 - experts :]
    total = own[...]
    for piece in pieces:
        total = total + piece[...].astype(jnp.float32)
    rounded = (resid[...].astype(jnp.float32) + total).astype(jnp.bfloat16)
    stream[...] = rounded
    wide = rounded.astype(jnp.float32)
    scale = lax.rsqrt(jnp.mean(wide * wide, axis=1, keepdims=True) + EPSILON)
    normed = (wide * scale * gain[...]).astype(jnp.bfloat16)
    rows = resid.shape[0]
    stride = padded(blocks[0].shape[0])
    numbers = lax.broadcasted_iota(jnp.int32, (len(blocks) * stride, rows), 0)
    hit = (numbers == slots[0:1, :]) | (numbers == slots[1:2, :])
    picked = jnp.dot(
        hit.astype(jnp.float32).astype(jnp.bfloat16), normed, preferred_element_type=jnp.float32
    ).astype(jnp.bfloat16)
    for i, block in enumerate(blocks):
        block[...] = picked[i * stride : i * stride + block.shape[0]]


def send_rows(resid, own, pieces, gain, slots, experts, capacity):
    rows, width = resid.shape
    block = jax.ShapeDtypeStruct((capacity, width), jnp.bfloat16)
    stream, *blocks = pl.pallas_call(
        functools.partial(send_kernel, experts=experts),
        out_shape=[jax.ShapeDtypeStruct((rows, width), jnp.bfloat16)] + [block] * experts,
        cost_estimate=pl.CostEstimate(
            flops=2 * rows * width * experts * capacity,
            bytes_accessed=8 * rows * width,
            transcendentals=0,
        ),
        compiler_params=granted(14),
        name="send_rows",
    )(resid, own, gain, slots, *pieces)
    return stream, blocks


def expert_kernel(place, *refs, groups, outs, pairs):
    rows_in, refs = refs[:groups], refs[groups:]
    (gate_own, up_own, gate_far, up_far, *downs), refs = refs[: 4 + 2 * pairs], refs[4 + 2 * pairs :]
    rows_out, (left, active) = refs[:outs], refs[outs:]
    hidden = gate_own.shape[1]
    strip, width = 2 * hidden, downs[0].shape[1]
    at = 0
    for block in rows_in:
        left[at : at + block.shape[0], :] = block[...]
        at += block.shape[0]
    step = min(256, hidden)
    for side, (gates, ups) in enumerate(((gate_own, up_own), (gate_far, up_far))):
        core = place[1] if side == 0 else 1 - place[1]
        for start in range(0, hidden, step):
            here = slice(start, start + step)
            gate = jnp.dot(left[...], gates[:, here], preferred_element_type=jnp.float32)
            upward = jnp.dot(left[...], ups[:, here], preferred_element_type=jnp.float32)
            there = pl.ds(pl.multiple_of(core * hidden + start, step), step)
            active[:, there] = (jax.nn.silu(gate) * upward).astype(jnp.bfloat16)
    for i, down in enumerate(downs):
        if i < 2:
            side, d = i, 0
            piece = down[pl.ds(pl.multiple_of(place[0] * strip, strip), strip), :]
        else:
            side, d = (i - 2) // (pairs - 1), (i - 2) % (pairs - 1) + 1
            piece = down[...]
        core = place[1] if side == 0 else 1 - place[1]
        column = (lax.rem(place[0] - d + pairs, pairs) * 2 + core) * width
        there = pl.ds(pl.multiple_of(column, width), width)
        result = jnp.dot(active[...], piece, preferred_element_type=jnp.float32)
        at = 0
        for block in rows_out:
            block[:, there] = result[at : at + block.shape[0]].astype(block.dtype)
            at += block.shape[0]


def expert_rows(place, rows, outs, weights):
    *gates, downs = weights
    model, hidden = gates[0].shape
    pairs = len(downs) // 2
    height = sum(a.shape[0] for a in rows)
    vmem = pl.BlockSpec(memory_space=pltpu.VMEM)
    return pl.pallas_call(
        functools.partial(expert_kernel, groups=len(rows), outs=len(outs), pairs=pairs),
        in_specs=[pl.BlockSpec(memory_space=pltpu.SMEM)]
        + [vmem] * (len(rows) + 4 + 2 * pairs),
        out_specs=[vmem] * len(outs),
        out_shape=[jax.ShapeDtypeStruct((count, model), kind) for count, kind in outs],
        scratch_shapes=[
            pltpu.VMEM((height, model), jnp.bfloat16),
            pltpu.VMEM((height, 2 * hidden), jnp.bfloat16),
        ],
        cost_estimate=pl.CostEstimate(
            flops=12 * height * model * hidden,
            bytes_accessed=12 * model * hidden,
            transcendentals=0,
        ),
        compiler_params=granted(28),
        name="expert_rows",
    )(place, *rows, *gates, *downs)


def mix_kernel(slots, pair_weight, mix):
    rows = slots.shape[0]
    numbers = lax.broadcasted_iota(jnp.int32, (rows, mix.shape[1]), 1)
    share = jnp.where(numbers == slots[:, 0:1], pair_weight[:, 0:1], 0.0)
    share = share + jnp.where(numbers == slots[:, 1:2], pair_weight[:, 1:2], 0.0)
    high = share.astype(jnp.bfloat16)
    mix[0:rows, :] = high
    mix[rows : 2 * rows, :] = (share - high.astype(jnp.float32)).astype(jnp.bfloat16)


def mix_weights(slots, pair_weight, count):
    return pl.pallas_call(
        mix_kernel,
        out_shape=jax.ShapeDtypeStruct((2 * slots.shape[0], count), jnp.bfloat16),
        compiler_params=granted(4),
        name="mix_weights",
    )(slots, pair_weight)


def blend_kernel(stream, mix, *refs):
    blocks, (out, table) = refs[:-2], refs[-2:]
    rows = stream.shape[0]
    stride = padded(blocks[0].shape[0])
    if stride != blocks[0].shape[0]:
        table[...] = jnp.zeros(table.shape, table.dtype)
    for i, block in enumerate(blocks):
        table[i * stride : i * stride + block.shape[0], :] = block[...]
    halves = jnp.dot(mix[...], table[...], preferred_element_type=jnp.float32)
    blended = halves[0:rows] + halves[rows:]
    out[...] = (stream[...].astype(jnp.float32) + blended).astype(jnp.bfloat16)


def blend_rows(stream, mix, blocks):
    rows, width = stream.shape
    lanes = min(1024, width)
    column = lambda count: pl.BlockSpec((count, lanes), lambda i: (0, i))
    fixed = lambda a: pl.BlockSpec(a.shape, lambda i: (0, 0))
    height = len(blocks) * padded(blocks[0].shape[0])
    return pl.pallas_call(
        blend_kernel,
        grid=(width // lanes,),
        in_specs=[column(rows), fixed(mix)] + [column(b.shape[0]) for b in blocks],
        out_specs=column(rows),
        out_shape=jax.ShapeDtypeStruct((rows, width), jnp.bfloat16),
        scratch_shapes=[pltpu.VMEM((height, lanes), jnp.bfloat16)],
        cost_estimate=pl.CostEstimate(
            flops=4 * rows * width * height, bytes_accessed=10 * rows * width, transcendentals=0
        ),
        compiler_params=granted(14),
        name="blend_rows",
    )(stream, mix, *blocks)


def slot_numbers(picks, experts):
    flat = picks.reshape(-1)
    onehot = (flat[:, None] == jnp.arange(experts, dtype=jnp.int32)[None, :]).astype(jnp.int32)
    before = jnp.cumsum(onehot, axis=0) - onehot
    return (flat, jnp.sum(before * onehot, axis=1))


def entering_state(total, me):
    size = lax.axis_size("sp")
    a, b = total[0:1], total[1:2]
    before = jnp.zeros_like(b)
    passed = jnp.ones_like(a)
    bit = 1
    while bit < size:
        other = across(jnp.concatenate([a, b], axis=0), bit)
        oa, ob = other[0:1], other[1:2]
        after = (me & bit) != 0
        before = jnp.where(after, passed * ob + before, before)
        passed = jnp.where(after, passed * oa, passed)
        b = jnp.where(after, a * ob + b, oa * b + ob)
        a = a * oa
        bit *= 2
    return before


def body(
    resid,
    recurrent_input,
    recurrent_out_gate,
    filter_weight,
    recurrence_gate_matrix,
    input_gate_matrix,
    channel_decay_raw,
    token_decay_boost,
    output_projection_weight,
    expert_norm_gain,
    routes,
    expert_pair_weight,
    gate_weight,
    up_weight,
    down_weight,
):
    tokens_here = recurrent_input.shape[0]
    tp_size, experts = lax.axis_size("tp"), lax.axis_size("sp")
    me, column = lax.axis_index("sp"), lax.axis_index("tp")
    pairs = tp_size // 2
    row, core = column // 2, column % 2
    place = jnp.stack([row, core]).astype(jnp.int32)
    rows_dev = tokens_here // tp_size
    capacity = max(2, 3 * rows_dev // experts)

    gate_own, up_own, down_all = gate_weight[0], up_weight[0], down_weight[0]
    strip = down_all.shape[0] // pairs
    strip_of = lambda d: lax.dynamic_slice_in_dim(down_all, lax.rem(row + d, pairs) * strip, strip, 0)
    rim = shifted(recurrent_input[tokens_here - 8 :])
    down_own = [turned(strip_of(d), d) for d in range(1, pairs)]
    projection_far = swapped(output_projection_weight)
    gate_far, up_far = swapped(gate_own), swapped(up_own)
    down_far = [swapped(piece) for piece in down_own]
    down_whole = [down_all, swapped(down_all)]
    weights = (gate_own, up_own, gate_far, up_far, down_whole + down_own + down_far)

    local, running, total = local_scan(
        rim,
        recurrent_input,
        filter_weight,
        recurrence_gate_matrix,
        input_gate_matrix,
        channel_decay_raw[None, :],
        token_decay_boost,
    )

    own_routes = lax.dynamic_slice_in_dim(routes, column * rows_dev, rows_dev, 0)
    own_flat, own_rank = slot_numbers(own_routes, experts)
    slots = ((own_flat ^ me) * padded(capacity) + own_rank).reshape(rows_dev, 2)

    before = entering_state(total, me)
    keep, give = finish_branch(place, before, local, running, recurrent_out_gate, pairs)
    taken = swapped(give)

    def projected(d):
        near = jnp.dot(keep[d], output_projection_weight, preferred_element_type=jnp.float32)
        return near + jnp.dot(taken[d], projection_far, preferred_element_type=jnp.float32)

    pieces = [turned(projected(d).astype(jnp.bfloat16), d) for d in range(1, pairs)]
    stream, blocks = send_rows(
        resid,
        projected(0),
        pieces,
        expert_norm_gain[None, :],
        slots.T,
        experts,
        capacity,
    )
    cuts = row_cuts(experts)
    arrived = {0: blocks[0]}
    for k in range(1, experts):
        arrived[k] = across(blocks[k], k)
    own = [jnp.concatenate([arrived[k] for k in range(*cut)], axis=0) for cut in cuts]
    theirs = [[turned(g, d) for d in range(1, pairs)] for g in own]
    hops = range(1, pairs)
    splits = return_cuts(experts)

    def run(chosen):
        rows = [own[i] for i in chosen] + [g for i in chosen for g in theirs[i]]
        outs = []
        for kind, count in ((jnp.float32, 1), (jnp.bfloat16, pairs - 1)):
            for i in chosen:
                parts = [((b - a) * capacity, kind) for a, b in splits if cuts[i][0] <= a < cuts[i][1]]
                outs += parts * count
        results = iter(expert_rows(place, rows, outs, weights))
        wide = {s: next(results) for i in chosen for s in inner(i)}
        narrow = {s: [] for i in chosen for s in inner(i)}
        for i in chosen:
            for _ in hops:
                for s in inner(i):
                    narrow[s].append(next(results))
        return wide, narrow

    def inner(i):
        return [s for s in splits if cuts[i][0] <= s[0] < cuts[i][1]]

    returned = {}
    for chosen in ((0, 1), (2,), (3,)):
        wide, narrow = run(chosen)
        for cut in wide:
            sums = wide[cut]
            for d in hops:
                back = turned(narrow[cut][d - 1], pairs - d)
                sums = sums + back.astype(jnp.float32)
            for j, k in enumerate(range(*cut)):
                result = sums[j * capacity : (j + 1) * capacity].astype(jnp.bfloat16)
                returned[k] = across(result, k) if k else result
    mix = mix_weights(slots, expert_pair_weight, experts * padded(capacity))
    return blend_rows(stream, mix, [returned[k] for k in range(experts)])


def row_cuts(experts):
    quarter = experts // 4
    return [(0, 1), (1, 2 * quarter), (2 * quarter, 3 * quarter), (3 * quarter, experts)]


def return_cuts(experts):
    first, near, far, last = row_cuts(experts)
    middle = (far[0] + far[1]) // 2
    return [first, near, (far[0], middle), (middle, far[1]), last]


def solution(mesh):
    placed = (
        P(("sp", "tp"), None),
        P("sp", "tp"),
        P("sp", "tp"),
        P(None, "tp"),
        P("tp", None, None),
        P("tp", None, None),
        P("tp"),
        P("sp", "tp"),
        P("tp", None),
        P(),
        P("sp", None),
        P(("sp", "tp"), None),
        P("sp", None, "tp"),
        P("sp", None, "tp"),
        P("sp", None, "tp"),
    )

    return jax.shard_map(
        body, mesh=mesh, in_specs=placed, out_specs=P(("sp", "tp"), None), check_vma=False
    )
```

```python
import functools

import jax
import jax.numpy as jnp
from jax import lax
from jax.experimental import pallas as pl
from jax.experimental.pallas import tpu as pltpu
from jax.sharding import PartitionSpec as P


RECURRENT_SCALE = 8.0
EPSILON = 1e-06


def granted(mebibytes):
    return pltpu.CompilerParams(vmem_limit_bytes=mebibytes * 2**20)


def shifted(block):
    size = lax.axis_size("sp")
    return lax.ppermute(block, "sp", [(i, i + 1) for i in range(size - 1)])


def across(block, bits):
    return lax.ppermute(block, "sp", [(i, i ^ bits) for i in range(lax.axis_size("sp"))])


def swapped(block):
    return lax.ppermute(block, "tp", [(i, i ^ 1) for i in range(lax.axis_size("tp"))])


def turned(block, distance):
    size = lax.axis_size("tp")
    return lax.ppermute(block, "tp", [(i, (i + 2 * distance) % size) for i in range(size)])


LANES = 128
GROUPS = 2
GRANT = 12
SEGMENTS = 8


def block_diagonal(blocks):
    count, width, _ = blocks.shape
    empty = jnp.zeros((width, width), blocks.dtype)
    rows = []
    for i in range(count):
        rows.append(jnp.concatenate([blocks[i] if j == i else empty for j in range(count)], axis=1))
    return jnp.concatenate(rows, axis=0)


def scan_kernel(place, rim, x, taps, recur, inward, slope, boost, down, local, running, total, *refs):
    *halves, wide, decays, drives, held, cut, kept = refs
    pairs = len(halves) // 2 + 1
    rows = halves[0].shape[0]
    loads, stores = [], []
    for i, half in enumerate(halves):
        target = lax.rem(place[0] + i // 2 + 1, pairs)
        begin = pl.multiple_of((2 * target + i % 2) * rows, rows)
        loads.append(pltpu.make_async_copy(down.at[pl.ds(begin, rows)], held.at[i], cut.at[i]))
        stores.append(pltpu.make_async_copy(held.at[i], half, kept.at[i]))
    final = pl.program_id(0) == pl.num_programs(0) - 1

    @pl.when(pl.program_id(0) == 0)
    def _():
        for copy in loads:
            copy.start()

    @pl.when(final)
    def _():
        for load, store in zip(loads, stores):
            load.wait()
            store.start()

    tokens, _ = x.shape
    margin = rim.shape[0]
    count = taps.shape[0]
    wide[0:margin, :] = rim[...].astype(jnp.float32)
    wide[margin : margin + tokens, :] = x[...].astype(jnp.float32)
    first = margin - count + 1
    mixed = wide[first : first + tokens, :] * taps[0:1, :]
    for j in range(1, count):
        mixed = mixed + wide[first + j : first + j + tokens, :] * taps[j : j + 1, :]
    smoothed = mixed.astype(jnp.bfloat16)
    recur_gate = jax.nn.sigmoid(
        jnp.dot(smoothed, block_diagonal(recur), preferred_element_type=jnp.float32)
    )
    input_gate = jax.nn.sigmoid(
        jnp.dot(smoothed, block_diagonal(inward), preferred_element_type=jnp.float32)
    )
    log_decay = -RECURRENT_SCALE * recur_gate * jax.nn.softplus(-slope[...]) + boost[...]
    decay = jnp.exp(log_decay)
    twice = 2.0 * log_decay
    series = 1.0 + twice * (1.0 / 9.0)
    for n in range(8, 1, -1):
        series = 1.0 + twice * (1.0 / n) * series
    lost = jnp.where(twice > -0.35, -twice * series, 1.0 - decay * decay)
    drive = jnp.sqrt(lost) * (input_gate * smoothed.astype(jnp.float32))
    groups, width = decays.shape[0], decays.shape[2]
    for g in range(groups):
        decays[g] = decay[:, g * width : (g + 1) * width]
        drives[g] = drive[:, g * width : (g + 1) * width]
    length = tokens // SEGMENTS

    def step(j, held):
        here = pl.ds(j, SEGMENTS, stride=length)
        after = []
        for g, (product, state) in enumerate(held):
            a = decays[g, here, :]
            state = a * state + drives[g, here, :]
            product = product * a
            local[g, here, :] = state
            running[g, here, :] = product
            after.append((product, state))
        return tuple(after)

    start = (jnp.ones((SEGMENTS, width), jnp.float32), jnp.zeros((SEGMENTS, width), jnp.float32))
    ends = lax.fori_loop(0, length, step, (start,) * groups, unroll=8)
    for g, (product, state) in enumerate(ends):
        a, b = product[0:1], state[0:1]
        for k in range(1, SEGMENTS):
            a, b = a * product[k : k + 1], product[k : k + 1] * b + state[k : k + 1]
        total[0:1, g * width : (g + 1) * width] = a
        total[1:2, g * width : (g + 1) * width] = b

    @pl.when(final)
    def _():
        for store in stores:
            store.wait()


def local_scan(place, rim, x, taps, recur, inward, slope, boost, down, pairs):
    tokens, channels = x.shape
    groups = min(GROUPS, channels // LANES)
    lanes = groups * LANES
    width = recur.shape[1]
    folded = pl.BlockSpec((groups, tokens, LANES), lambda i: (i, 0, 0))
    anywhere = pl.BlockSpec(memory_space=pl.ANY)
    count = 2 * (pairs - 1)
    half = jax.ShapeDtypeStruct((down.shape[0] // (2 * pairs), down.shape[1]), down.dtype)
    column = lambda rows: pl.BlockSpec((rows, lanes), lambda i: (0, i))
    blocks = pl.BlockSpec((lanes // width, width, width), lambda i: (i, 0, 0))
    wide = jax.ShapeDtypeStruct((channels // LANES, tokens, LANES), jnp.float32)
    return pl.pallas_call(
        scan_kernel,
        grid=(channels // lanes,),
        in_specs=[
            pl.BlockSpec(memory_space=pltpu.SMEM),
            column(rim.shape[0]),
            column(tokens),
            column(taps.shape[0]),
            blocks,
            blocks,
            column(1),
            column(tokens),
            anywhere,
        ],
        out_specs=[folded, folded, column(2)] + [anywhere] * count,
        out_shape=[wide, wide, jax.ShapeDtypeStruct((2, channels), jnp.float32)] + [half] * count,
        scratch_shapes=[
            pltpu.VMEM((tokens + rim.shape[0], lanes), jnp.float32),
            pltpu.VMEM((groups, tokens, LANES), jnp.float32),
            pltpu.VMEM((groups, tokens, LANES), jnp.float32),
            pltpu.VMEM((count, *half.shape), half.dtype),
            pltpu.SemaphoreType.DMA((count,)),
            pltpu.SemaphoreType.DMA((count,)),
        ],
        name="local_scan",
    )(place, rim, x, taps, recur, inward, slope, boost, down)


def branch_kernel(place, entering, local, running, gate, keep, give):
    groups, tokens, width = local.shape
    length = tokens // SEGMENTS
    pairs, rows = keep.shape[0], keep.shape[1]
    step = min(length, rows)
    begins = [entering[:, g * width : (g + 1) * width] for g in range(groups)]
    for start in range(0, tokens, step):
        here = slice(start, start + step)
        states = [local[g, here, :] + running[g, here, :] * begins[g] for g in range(groups)]
        opened = jax.nn.gelu(gate[here, :].astype(jnp.float32))
        value = (opened * jnp.concatenate(states, axis=1)).astype(jnp.bfloat16)
        block = start // rows
        slot = lax.rem(block // 2 - place[0] + pairs, pairs)
        inside = slice(start % rows, start % rows + step)
        mine = place[1] == block % 2

        @pl.when(mine)
        def _():
            keep[slot, inside, :] = value

        @pl.when(jnp.logical_not(mine))
        def _():
            give[slot, inside, :] = value

        if (start + step) % length == 0:
            begins = [state[step - 1 : step] for state in states]


def finish_branch(place, entering, local, running, gate, pairs):
    tokens, channels = gate.shape
    groups = min(GROUPS, channels // LANES)
    lanes = groups * LANES
    column = lambda rows: pl.BlockSpec((rows, lanes), lambda i: (0, i))
    folded = pl.BlockSpec((groups, tokens, LANES), lambda i: (i, 0, 0))
    rows = tokens // (2 * pairs)
    half = jax.ShapeDtypeStruct((pairs, rows, channels), jnp.bfloat16)
    return pl.pallas_call(
        branch_kernel,
        grid=(channels // lanes,),
        in_specs=[
            pl.BlockSpec(memory_space=pltpu.SMEM),
            column(1),
            folded,
            folded,
            column(tokens),
        ],
        out_specs=[pl.BlockSpec((pairs, rows, lanes), lambda i: (0, 0, i))] * 2,
        out_shape=[half, half],
        cost_estimate=pl.CostEstimate(
            flops=20 * tokens * channels, bytes_accessed=12 * tokens * channels, transcendentals=0
        ),
        name="finish_branch",
    )(place, entering, local, running, gate)


def padded(count):
    return -(-count // 16) * 16


def send_kernel(resid, own, gain, slots, *refs, experts):
    pieces, (stream, *blocks) = refs[: -1 - experts], refs[-1 - experts :]
    total = own[...]
    for piece in pieces:
        total = total + piece[...].astype(jnp.float32)
    rounded = (resid[...].astype(jnp.float32) + total).astype(jnp.bfloat16)
    stream[...] = rounded
    wide = rounded.astype(jnp.float32)
    scale = lax.rsqrt(jnp.mean(wide * wide, axis=1, keepdims=True) + EPSILON)
    normed = (wide * scale * gain[...]).astype(jnp.bfloat16)
    rows = resid.shape[0]
    stride = padded(blocks[0].shape[0])
    numbers = lax.broadcasted_iota(jnp.int32, (len(blocks) * stride, rows), 0)
    hit = (numbers == slots[0:1, :]) | (numbers == slots[1:2, :])
    picked = jnp.dot(
        hit.astype(jnp.float32).astype(jnp.bfloat16), normed, preferred_element_type=jnp.float32
    ).astype(jnp.bfloat16)
    for i, block in enumerate(blocks):
        block[...] = picked[i * stride : i * stride + block.shape[0]]


def send_rows(resid, own, pieces, gain, slots, experts, capacity):
    rows, width = resid.shape
    block = jax.ShapeDtypeStruct((capacity, width), jnp.bfloat16)
    stream, *blocks = pl.pallas_call(
        functools.partial(send_kernel, experts=experts),
        out_shape=[jax.ShapeDtypeStruct((rows, width), jnp.bfloat16)] + [block] * experts,
        cost_estimate=pl.CostEstimate(
            flops=2 * rows * width * experts * capacity,
            bytes_accessed=8 * rows * width,
            transcendentals=0,
        ),
        compiler_params=granted(14),
        name="send_rows",
    )(resid, own, gain, slots, *pieces)
    return stream, blocks


def expert_kernel(place, *refs, groups, outs, pairs):
    rows_in, refs = refs[:groups], refs[groups:]
    used = 2 + 4 * pairs
    (gate_own, up_own, gate_far, up_far, *downs), refs = refs[:used], refs[used:]
    rows_out, (left, active) = refs[:outs], refs[outs:]
    hidden = gate_own.shape[1]
    width = downs[0].shape[1]
    at = 0
    for block in rows_in:
        left[at : at + block.shape[0], :] = block[...]
        at += block.shape[0]
    step = min(256, hidden)
    for side, (gates, ups) in enumerate(((gate_own, up_own), (gate_far, up_far))):
        core = place[1] if side == 0 else 1 - place[1]
        for start in range(0, hidden, step):
            here = slice(start, start + step)
            gate = jnp.dot(left[...], gates[:, here], preferred_element_type=jnp.float32)
            upward = jnp.dot(left[...], ups[:, here], preferred_element_type=jnp.float32)
            there = pl.ds(pl.multiple_of(core * hidden + start, step), step)
            active[:, there] = (jax.nn.silu(gate) * upward).astype(jnp.bfloat16)
    for side in range(2):
        for d in range(pairs):
            core = place[1] if side == 0 else 1 - place[1]
            column = (lax.rem(place[0] - d + pairs, pairs) * 2 + core) * width
            there = pl.ds(pl.multiple_of(column, width), width)
            if d == 0:
                begin = pl.multiple_of(place[0] * 2 * hidden, 2 * hidden)
                piece = downs[side][pl.ds(begin, 2 * hidden), :]
                result = jnp.dot(active[...], piece, preferred_element_type=jnp.float32)
            else:
                first, second = downs[2 + 2 * (pairs - 1) * side + 2 * d - 2 :][:2]
                result = jnp.dot(
                    active[:, :hidden], first[...], preferred_element_type=jnp.float32
                ) + jnp.dot(active[:, hidden:], second[...], preferred_element_type=jnp.float32)
            at = 0
            for block in rows_out:
                block[:, there] = result[at : at + block.shape[0]].astype(block.dtype)
                at += block.shape[0]


def expert_rows(place, rows, outs, weights):
    *gates, downs = weights
    model, hidden = gates[0].shape
    pairs = (len(downs) + 2) // 4
    height = sum(a.shape[0] for a in rows)
    vmem = pl.BlockSpec(memory_space=pltpu.VMEM)
    return pl.pallas_call(
        functools.partial(expert_kernel, groups=len(rows), outs=len(outs), pairs=pairs),
        in_specs=[pl.BlockSpec(memory_space=pltpu.SMEM)]
        + [vmem] * (len(rows) + 4 + len(downs)),
        out_specs=[vmem] * len(outs),
        out_shape=[jax.ShapeDtypeStruct((count, model), kind) for count, kind in outs],
        scratch_shapes=[
            pltpu.VMEM((height, model), jnp.bfloat16),
            pltpu.VMEM((height, 2 * hidden), jnp.bfloat16),
        ],
        cost_estimate=pl.CostEstimate(
            flops=12 * height * model * hidden,
            bytes_accessed=12 * model * hidden,
            transcendentals=0,
        ),
        compiler_params=granted(GRANT),
        name="expert_rows",
    )(place, *rows, *gates, *downs)


def sum_kernel(own, *refs, pieces):
    backs, blocks = refs[:pieces], refs[pieces:]
    total = own[...]
    for back in backs:
        total = total + back[...].astype(jnp.float32)
    height = blocks[0].shape[0]
    for i, block in enumerate(blocks):
        block[...] = total[i * height : (i + 1) * height].astype(jnp.bfloat16)


def sum_rows(own, backs, count):
    rows, width = own.shape
    block = jax.ShapeDtypeStruct((rows // count, width), jnp.bfloat16)
    return pl.pallas_call(
        functools.partial(sum_kernel, pieces=len(backs)),
        out_shape=[block] * count,
        cost_estimate=pl.CostEstimate(
            flops=2 * rows * width, bytes_accessed=8 * rows * width, transcendentals=0
        ),
        compiler_params=granted(8),
        name="sum_rows",
    )(own, *backs)


def mix_kernel(slots, pair_weight, mix):
    rows = slots.shape[0]
    numbers = lax.broadcasted_iota(jnp.int32, (rows, mix.shape[1]), 1)
    share = jnp.where(numbers == slots[:, 0:1], pair_weight[:, 0:1], 0.0)
    share = share + jnp.where(numbers == slots[:, 1:2], pair_weight[:, 1:2], 0.0)
    high = share.astype(jnp.bfloat16)
    mix[0:rows, :] = high
    mix[rows : 2 * rows, :] = (share - high.astype(jnp.float32)).astype(jnp.bfloat16)


def mix_weights(slots, pair_weight, count):
    return pl.pallas_call(
        mix_kernel,
        out_shape=jax.ShapeDtypeStruct((2 * slots.shape[0], count), jnp.bfloat16),
        compiler_params=granted(4),
        name="mix_weights",
    )(slots, pair_weight)


def blend_kernel(stream, mix, *refs):
    blocks, (out, table) = refs[:-2], refs[-2:]
    rows = stream.shape[0]
    stride = padded(blocks[0].shape[0])
    if stride != blocks[0].shape[0]:
        table[...] = jnp.zeros(table.shape, table.dtype)
    for i, block in enumerate(blocks):
        table[i * stride : i * stride + block.shape[0], :] = block[...]
    halves = jnp.dot(mix[...], table[...], preferred_element_type=jnp.float32)
    blended = halves[0:rows] + halves[rows:]
    out[...] = (stream[...].astype(jnp.float32) + blended).astype(jnp.bfloat16)


def blend_rows(stream, mix, blocks):
    rows, width = stream.shape
    lanes = min(1024, width)
    column = lambda count: pl.BlockSpec((count, lanes), lambda i: (0, i))
    fixed = lambda a: pl.BlockSpec(a.shape, lambda i: (0, 0))
    height = len(blocks) * padded(blocks[0].shape[0])
    return pl.pallas_call(
        blend_kernel,
        grid=(width // lanes,),
        in_specs=[column(rows), fixed(mix)] + [column(b.shape[0]) for b in blocks],
        out_specs=column(rows),
        out_shape=jax.ShapeDtypeStruct((rows, width), jnp.bfloat16),
        scratch_shapes=[pltpu.VMEM((height, lanes), jnp.bfloat16)],
        cost_estimate=pl.CostEstimate(
            flops=4 * rows * width * height, bytes_accessed=10 * rows * width, transcendentals=0
        ),
        compiler_params=granted(14),
        name="blend_rows",
    )(stream, mix, *blocks)


def slot_numbers(picks, experts):
    flat = picks.reshape(-1)
    onehot = (flat[:, None] == jnp.arange(experts, dtype=jnp.int32)[None, :]).astype(jnp.int32)
    before = jnp.cumsum(onehot, axis=0) - onehot
    return (flat, jnp.sum(before * onehot, axis=1))


def entering_state(total, me):
    size = lax.axis_size("sp")
    a, b = total[0:1], total[1:2]
    before = jnp.zeros_like(b)
    passed = jnp.ones_like(a)
    bit = 1
    while bit < size:
        other = across(jnp.concatenate([a, b], axis=0), bit)
        oa, ob = other[0:1], other[1:2]
        after = (me & bit) != 0
        before = jnp.where(after, passed * ob + before, before)
        passed = jnp.where(after, passed * oa, passed)
        b = jnp.where(after, a * ob + b, oa * b + ob)
        a = a * oa
        bit *= 2
    return before


def body(
    resid,
    recurrent_input,
    recurrent_out_gate,
    filter_weight,
    recurrence_gate_matrix,
    input_gate_matrix,
    channel_decay_raw,
    token_decay_boost,
    output_projection_weight,
    expert_norm_gain,
    routes,
    expert_pair_weight,
    gate_weight,
    up_weight,
    down_weight,
):
    tokens_here = recurrent_input.shape[0]
    tp_size, experts = lax.axis_size("tp"), lax.axis_size("sp")
    me, column = lax.axis_index("sp"), lax.axis_index("tp")
    pairs = tp_size // 2
    row, core = column // 2, column % 2
    place = jnp.stack([row, core]).astype(jnp.int32)
    rows_dev = tokens_here // tp_size
    capacity = max(2, 3 * rows_dev // experts)

    gate_own, up_own, down_all = gate_weight[0], up_weight[0], down_weight[0]
    rim = shifted(recurrent_input[tokens_here - 8 :])
    local, running, total, *halves = local_scan(
        place,
        rim,
        recurrent_input,
        filter_weight,
        recurrence_gate_matrix,
        input_gate_matrix,
        channel_decay_raw[None, :],
        token_decay_boost,
        down_all,
        pairs,
    )
    projection_far = swapped(output_projection_weight)
    gate_far, up_far = swapped(gate_own), swapped(up_own)
    down_own, down_far = [], []
    for d in range(1, pairs):
        for h in range(2):
            down_own.append(turned(halves[2 * d - 2 + h], d))
            down_far.append(swapped(down_own[-1]))
    down_whole = [down_all, swapped(down_all)]
    weights = (gate_own, up_own, gate_far, up_far, down_whole + down_own + down_far)

    own_routes = lax.dynamic_slice_in_dim(routes, column * rows_dev, rows_dev, 0)
    own_flat, own_rank = slot_numbers(own_routes, experts)
    slots = ((own_flat ^ me) * padded(capacity) + own_rank).reshape(rows_dev, 2)

    before = entering_state(total, me)
    keep, give = finish_branch(place, before, local, running, recurrent_out_gate, pairs)
    taken = swapped(give)

    def projected(d):
        near = jnp.dot(keep[d], output_projection_weight, preferred_element_type=jnp.float32)
        return near + jnp.dot(taken[d], projection_far, preferred_element_type=jnp.float32)

    pieces = [turned(projected(d).astype(jnp.bfloat16), d) for d in range(1, pairs)]
    stream, blocks = send_rows(
        resid,
        projected(0),
        pieces,
        expert_norm_gain[None, :],
        slots.T,
        experts,
        capacity,
    )
    cuts = row_cuts(experts)
    arrived = {0: blocks[0]}
    for k in range(1, experts):
        arrived[k] = across(blocks[k], k)
    own = [joined([arrived[k] for k in range(*cut)]) for cut in cuts]
    theirs = [[turned(g, d) for d in range(1, pairs)] for g in own]
    hops = range(1, pairs)
    sizes = [(cut[1] - cut[0]) * capacity for cut in cuts]
    returned = {}
    near, mid = len(cuts) // 2, 3 * len(cuts) // 4
    calls = [(0, near), (near, mid), (mid, len(cuts))]
    for first, end in calls:
        chosen = range(first, end)
        rows = [own[i] for i in chosen] + [g for i in chosen for g in theirs[i]]
        outs = [(sizes[i], jnp.float32) for i in chosen]
        outs += [(sizes[i], jnp.bfloat16) for i in chosen for _ in hops]
        results = expert_rows(place, rows, outs, weights)
        wide, narrow = results[: len(chosen)], results[len(chosen) :]
        for j, i in enumerate(chosen):
            parts = narrow[j * len(hops) : (j + 1) * len(hops)]
            backs = [turned(part, pairs - d) for part, d in zip(parts, hops)]
            sums = sum_rows(wide[j], backs, cuts[i][1] - cuts[i][0])
            for k, result in zip(range(*cuts[i]), sums):
                returned[k] = across(result, k) if k else result
    mix = mix_weights(slots, expert_pair_weight, experts * padded(capacity))
    return blend_rows(stream, mix, [returned[k] for k in range(experts)])


def joined(blocks):
    return blocks[0] if len(blocks) == 1 else jnp.concatenate(blocks, axis=0)


def row_cuts(experts):
    count = max(1, experts // 8)
    return [(k, k + count) for k in range(0, experts, count)]


def solution(mesh):
    placed = (
        P(("sp", "tp"), None),
        P("sp", "tp"),
        P("sp", "tp"),
        P(None, "tp"),
        P("tp", None, None),
        P("tp", None, None),
        P("tp"),
        P("sp", "tp"),
        P("tp", None),
        P(),
        P("sp", None),
        P(("sp", "tp"), None),
        P("sp", None, "tp"),
        P("sp", None, "tp"),
        P("sp", None, "tp"),
    )

    return jax.shard_map(
        body, mesh=mesh, in_specs=placed, out_specs=P(("sp", "tp"), None), check_vma=False
    )
```

```python
import functools

import jax
import jax.numpy as jnp
from jax import lax
from jax.experimental import pallas as pl
from jax.experimental.pallas import tpu as pltpu
from jax.sharding import PartitionSpec as P


RECURRENT_SCALE = 8.0
EPSILON = 1e-06


def granted(mebibytes):
    return pltpu.CompilerParams(vmem_limit_bytes=mebibytes * 2**20)


def shifted(block):
    size = lax.axis_size("sp")
    return lax.ppermute(block, "sp", [(i, i + 1) for i in range(size - 1)])


def across(block, bits):
    return lax.ppermute(block, "sp", [(i, i ^ bits) for i in range(lax.axis_size("sp"))])


def swapped(block):
    return lax.ppermute(block, "tp", [(i, i ^ 1) for i in range(lax.axis_size("tp"))])


def turned(block, distance):
    size = lax.axis_size("tp")
    return lax.ppermute(block, "tp", [(i, (i + 2 * distance) % size) for i in range(size)])


LANES = 128
GROUPS = 2
GRANT = 12
SEGMENTS = 8


def block_diagonal(blocks):
    count, width, _ = blocks.shape
    empty = jnp.zeros((width, width), blocks.dtype)
    rows = []
    for i in range(count):
        rows.append(jnp.concatenate([blocks[i] if j == i else empty for j in range(count)], axis=1))
    return jnp.concatenate(rows, axis=0)


def scan_kernel(place, rim, x, taps, recur, inward, slope, boost, down, local, running, total, *refs):
    *halves, wide, decays, drives, held, cut, kept = refs
    pairs = len(halves) // 2 + 1
    rows = halves[0].shape[0]
    loads, stores = [], []
    for i, half in enumerate(halves):
        target = lax.rem(place[0] + i // 2 + 1, pairs)
        begin = pl.multiple_of((2 * target + i % 2) * rows, rows)
        loads.append(pltpu.make_async_copy(down.at[pl.ds(begin, rows)], held.at[i], cut.at[i]))
        stores.append(pltpu.make_async_copy(held.at[i], half, kept.at[i]))
    final = pl.program_id(0) == pl.num_programs(0) - 1

    @pl.when(pl.program_id(0) == 0)
    def _():
        for copy in loads:
            copy.start()

    @pl.when(final)
    def _():
        for load, store in zip(loads, stores):
            load.wait()
            store.start()

    tokens, _ = x.shape
    margin = rim.shape[0]
    count = taps.shape[0]
    wide[0:margin, :] = rim[...].astype(jnp.float32)
    wide[margin : margin + tokens, :] = x[...].astype(jnp.float32)
    first = margin - count + 1
    mixed = wide[first : first + tokens, :] * taps[0:1, :]
    for j in range(1, count):
        mixed = mixed + wide[first + j : first + j + tokens, :] * taps[j : j + 1, :]
    smoothed = mixed.astype(jnp.bfloat16)
    recur_gate = jax.nn.sigmoid(
        jnp.dot(smoothed, block_diagonal(recur), preferred_element_type=jnp.float32)
    )
    input_gate = jax.nn.sigmoid(
        jnp.dot(smoothed, block_diagonal(inward), preferred_element_type=jnp.float32)
    )
    log_decay = -RECURRENT_SCALE * recur_gate * jax.nn.softplus(-slope[...]) + boost[...]
    decay = jnp.exp(log_decay)
    twice = 2.0 * log_decay
    series = 1.0 + twice * (1.0 / 6.0)
    for n in range(5, 1, -1):
        series = 1.0 + twice * (1.0 / n) * series
    lost = jnp.where(twice > -0.1, -twice * series, 1.0 - decay * decay)
    drive = jnp.sqrt(lost) * (input_gate * smoothed.astype(jnp.float32))
    groups, width = decays.shape[0], decays.shape[2]
    for g in range(groups):
        decays[g] = decay[:, g * width : (g + 1) * width]
        drives[g] = drive[:, g * width : (g + 1) * width]
    length = tokens // SEGMENTS

    def step(j, held):
        here = pl.ds(j, SEGMENTS, stride=length)
        after = []
        for g, (product, state) in enumerate(held):
            a = decays[g, here, :]
            state = a * state + drives[g, here, :]
            product = product * a
            local[g, here, :] = state
            running[g, here, :] = product
            after.append((product, state))
        return tuple(after)

    start = (jnp.ones((SEGMENTS, width), jnp.float32), jnp.zeros((SEGMENTS, width), jnp.float32))
    ends = lax.fori_loop(0, length, step, (start,) * groups, unroll=8)
    for g, (product, state) in enumerate(ends):
        a, b = product[0:1], state[0:1]
        for k in range(1, SEGMENTS):
            a, b = a * product[k : k + 1], product[k : k + 1] * b + state[k : k + 1]
        total[0:1, g * width : (g + 1) * width] = a
        total[1:2, g * width : (g + 1) * width] = b

    @pl.when(final)
    def _():
        for store in stores:
            store.wait()


def local_scan(place, rim, x, taps, recur, inward, slope, boost, down, pairs):
    tokens, channels = x.shape
    groups = min(GROUPS, channels // LANES)
    lanes = groups * LANES
    width = recur.shape[1]
    folded = pl.BlockSpec((groups, tokens, LANES), lambda i: (i, 0, 0))
    anywhere = pl.BlockSpec(memory_space=pl.ANY)
    count = 2 * (pairs - 1)
    half = jax.ShapeDtypeStruct((down.shape[0] // (2 * pairs), down.shape[1]), down.dtype)
    column = lambda rows: pl.BlockSpec((rows, lanes), lambda i: (0, i))
    blocks = pl.BlockSpec((lanes // width, width, width), lambda i: (i, 0, 0))
    wide = jax.ShapeDtypeStruct((channels // LANES, tokens, LANES), jnp.float32)
    return pl.pallas_call(
        scan_kernel,
        grid=(channels // lanes,),
        in_specs=[
            pl.BlockSpec(memory_space=pltpu.SMEM),
            column(rim.shape[0]),
            column(tokens),
            column(taps.shape[0]),
            blocks,
            blocks,
            column(1),
            column(tokens),
            anywhere,
        ],
        out_specs=[folded, folded, column(2)] + [anywhere] * count,
        out_shape=[wide, wide, jax.ShapeDtypeStruct((2, channels), jnp.float32)] + [half] * count,
        scratch_shapes=[
            pltpu.VMEM((tokens + rim.shape[0], lanes), jnp.float32),
            pltpu.VMEM((groups, tokens, LANES), jnp.float32),
            pltpu.VMEM((groups, tokens, LANES), jnp.float32),
            pltpu.VMEM((count, *half.shape), half.dtype),
            pltpu.SemaphoreType.DMA((count,)),
            pltpu.SemaphoreType.DMA((count,)),
        ],
        name="local_scan",
    )(place, rim, x, taps, recur, inward, slope, boost, down)


def branch_kernel(place, entering, local, running, gate, keep, give):
    groups, tokens, width = local.shape
    length = tokens // SEGMENTS
    pairs, rows = keep.shape[0], keep.shape[1]
    step = min(length, rows)
    begins = [entering[:, g * width : (g + 1) * width] for g in range(groups)]
    for start in range(0, tokens, step):
        here = slice(start, start + step)
        states = [local[g, here, :] + running[g, here, :] * begins[g] for g in range(groups)]
        opened = jax.nn.gelu(gate[here, :].astype(jnp.float32))
        value = (opened * jnp.concatenate(states, axis=1)).astype(jnp.bfloat16)
        block = start // rows
        slot = lax.rem(block // 2 - place[0] + pairs, pairs)
        inside = slice(start % rows, start % rows + step)
        mine = place[1] == block % 2

        @pl.when(mine)
        def _():
            keep[slot, inside, :] = value

        @pl.when(jnp.logical_not(mine))
        def _():
            give[slot, inside, :] = value

        if (start + step) % length == 0:
            begins = [state[step - 1 : step] for state in states]


def finish_branch(place, entering, local, running, gate, pairs):
    tokens, channels = gate.shape
    groups = min(GROUPS, channels // LANES)
    lanes = groups * LANES
    column = lambda rows: pl.BlockSpec((rows, lanes), lambda i: (0, i))
    folded = pl.BlockSpec((groups, tokens, LANES), lambda i: (i, 0, 0))
    rows = tokens // (2 * pairs)
    half = jax.ShapeDtypeStruct((pairs, rows, channels), jnp.bfloat16)
    return pl.pallas_call(
        branch_kernel,
        grid=(channels // lanes,),
        in_specs=[
            pl.BlockSpec(memory_space=pltpu.SMEM),
            column(1),
            folded,
            folded,
            column(tokens),
        ],
        out_specs=[pl.BlockSpec((pairs, rows, lanes), lambda i: (0, 0, i))] * 2,
        out_shape=[half, half],
        cost_estimate=pl.CostEstimate(
            flops=20 * tokens * channels, bytes_accessed=12 * tokens * channels, transcendentals=0
        ),
        name="finish_branch",
    )(place, entering, local, running, gate)


def padded(count):
    return -(-count // 16) * 16


def send_kernel(resid, own, gain, slots, *refs, experts):
    pieces, (stream, *blocks) = refs[: -1 - experts], refs[-1 - experts :]
    total = own[...]
    for piece in pieces:
        total = total + piece[...].astype(jnp.float32)
    rounded = (resid[...].astype(jnp.float32) + total).astype(jnp.bfloat16)
    stream[...] = rounded
    wide = rounded.astype(jnp.float32)
    scale = lax.rsqrt(jnp.mean(wide * wide, axis=1, keepdims=True) + EPSILON)
    normed = (wide * scale * gain[...]).astype(jnp.bfloat16)
    rows = resid.shape[0]
    stride = padded(blocks[0].shape[0])
    numbers = lax.broadcasted_iota(jnp.int32, (len(blocks) * stride, rows), 0)
    hit = (numbers == slots[0:1, :]) | (numbers == slots[1:2, :])
    picked = jnp.dot(
        hit.astype(jnp.float32).astype(jnp.bfloat16), normed, preferred_element_type=jnp.float32
    ).astype(jnp.bfloat16)
    for i, block in enumerate(blocks):
        block[...] = picked[i * stride : i * stride + block.shape[0]]


def send_rows(resid, own, pieces, gain, slots, experts, capacity):
    rows, width = resid.shape
    block = jax.ShapeDtypeStruct((capacity, width), jnp.bfloat16)
    stream, *blocks = pl.pallas_call(
        functools.partial(send_kernel, experts=experts),
        out_shape=[jax.ShapeDtypeStruct((rows, width), jnp.bfloat16)] + [block] * experts,
        cost_estimate=pl.CostEstimate(
            flops=2 * rows * width * experts * capacity,
            bytes_accessed=8 * rows * width,
            transcendentals=0,
        ),
        compiler_params=granted(14),
        name="send_rows",
    )(resid, own, gain, slots, *pieces)
    return stream, blocks


def expert_kernel(place, *refs, groups, outs, pairs):
    rows_in, refs = refs[:groups], refs[groups:]
    used = 2 + 4 * pairs
    (gate_own, up_own, gate_far, up_far, *downs), refs = refs[:used], refs[used:]
    rows_out, (left, active) = refs[:outs], refs[outs:]
    hidden = gate_own.shape[1]
    width = downs[0].shape[1]
    at = 0
    for block in rows_in:
        left[at : at + block.shape[0], :] = block[...]
        at += block.shape[0]
    step = min(256, hidden)
    for side, (gates, ups) in enumerate(((gate_own, up_own), (gate_far, up_far))):
        core = place[1] if side == 0 else 1 - place[1]
        for start in range(0, hidden, step):
            here = slice(start, start + step)
            gate = jnp.dot(left[...], gates[:, here], preferred_element_type=jnp.float32)
            upward = jnp.dot(left[...], ups[:, here], preferred_element_type=jnp.float32)
            there = pl.ds(pl.multiple_of(core * hidden + start, step), step)
            active[:, there] = (jax.nn.silu(gate) * upward).astype(jnp.bfloat16)
    for side in range(2):
        for d in range(pairs):
            core = place[1] if side == 0 else 1 - place[1]
            column = (lax.rem(place[0] - d + pairs, pairs) * 2 + core) * width
            there = pl.ds(pl.multiple_of(column, width), width)
            if d == 0:
                begin = pl.multiple_of(place[0] * 2 * hidden, 2 * hidden)
                piece = downs[side][pl.ds(begin, 2 * hidden), :]
                result = jnp.dot(active[...], piece, preferred_element_type=jnp.float32)
            else:
                first, second = downs[2 + 2 * (pairs - 1) * side + 2 * d - 2 :][:2]
                result = jnp.dot(
                    active[:, :hidden], first[...], preferred_element_type=jnp.float32
                ) + jnp.dot(active[:, hidden:], second[...], preferred_element_type=jnp.float32)
            at = 0
            for block in rows_out:
                block[:, there] = result[at : at + block.shape[0]].astype(block.dtype)
                at += block.shape[0]


def expert_rows(place, rows, outs, weights):
    *gates, downs = weights
    model, hidden = gates[0].shape
    pairs = (len(downs) + 2) // 4
    height = sum(a.shape[0] for a in rows)
    vmem = pl.BlockSpec(memory_space=pltpu.VMEM)
    return pl.pallas_call(
        functools.partial(expert_kernel, groups=len(rows), outs=len(outs), pairs=pairs),
        in_specs=[pl.BlockSpec(memory_space=pltpu.SMEM)]
        + [vmem] * (len(rows) + 4 + len(downs)),
        out_specs=[vmem] * len(outs),
        out_shape=[jax.ShapeDtypeStruct((count, model), kind) for count, kind in outs],
        scratch_shapes=[
            pltpu.VMEM((height, model), jnp.bfloat16),
            pltpu.VMEM((height, 2 * hidden), jnp.bfloat16),
        ],
        cost_estimate=pl.CostEstimate(
            flops=12 * height * model * hidden,
            bytes_accessed=12 * model * hidden,
            transcendentals=0,
        ),
        compiler_params=granted(GRANT),
        name="expert_rows",
    )(place, *rows, *gates, *downs)


def sum_kernel(own, *refs, pieces):
    backs, blocks = refs[:pieces], refs[pieces:]
    total = own[...]
    for back in backs:
        total = total + back[...].astype(jnp.float32)
    height = blocks[0].shape[0]
    for i, block in enumerate(blocks):
        block[...] = total[i * height : (i + 1) * height].astype(jnp.bfloat16)


def sum_rows(own, backs, count):
    rows, width = own.shape
    block = jax.ShapeDtypeStruct((rows // count, width), jnp.bfloat16)
    return pl.pallas_call(
        functools.partial(sum_kernel, pieces=len(backs)),
        out_shape=[block] * count,
        cost_estimate=pl.CostEstimate(
            flops=2 * rows * width, bytes_accessed=8 * rows * width, transcendentals=0
        ),
        compiler_params=granted(8),
        name="sum_rows",
    )(own, *backs)


def mix_kernel(slots, pair_weight, mix):
    rows = slots.shape[0]
    numbers = lax.broadcasted_iota(jnp.int32, (rows, mix.shape[1]), 1)
    share = jnp.where(numbers == slots[:, 0:1], pair_weight[:, 0:1], 0.0)
    share = share + jnp.where(numbers == slots[:, 1:2], pair_weight[:, 1:2], 0.0)
    high = share.astype(jnp.bfloat16)
    mix[0:rows, :] = high
    mix[rows : 2 * rows, :] = (share - high.astype(jnp.float32)).astype(jnp.bfloat16)


def mix_weights(slots, pair_weight, count):
    return pl.pallas_call(
        mix_kernel,
        out_shape=jax.ShapeDtypeStruct((2 * slots.shape[0], count), jnp.bfloat16),
        compiler_params=granted(4),
        name="mix_weights",
    )(slots, pair_weight)


def blend_kernel(stream, mix, *refs):
    blocks, (out, table) = refs[:-2], refs[-2:]
    rows = stream.shape[0]
    stride = padded(blocks[0].shape[0])
    if stride != blocks[0].shape[0]:
        table[...] = jnp.zeros(table.shape, table.dtype)
    for i, block in enumerate(blocks):
        table[i * stride : i * stride + block.shape[0], :] = block[...]
    halves = jnp.dot(mix[...], table[...], preferred_element_type=jnp.float32)
    blended = halves[0:rows] + halves[rows:]
    out[...] = (stream[...].astype(jnp.float32) + blended).astype(jnp.bfloat16)


def blend_rows(stream, mix, blocks):
    rows, width = stream.shape
    lanes = min(1024, width)
    column = lambda count: pl.BlockSpec((count, lanes), lambda i: (0, i))
    fixed = lambda a: pl.BlockSpec(a.shape, lambda i: (0, 0))
    height = len(blocks) * padded(blocks[0].shape[0])
    return pl.pallas_call(
        blend_kernel,
        grid=(width // lanes,),
        in_specs=[column(rows), fixed(mix)] + [column(b.shape[0]) for b in blocks],
        out_specs=column(rows),
        out_shape=jax.ShapeDtypeStruct((rows, width), jnp.bfloat16),
        scratch_shapes=[pltpu.VMEM((height, lanes), jnp.bfloat16)],
        cost_estimate=pl.CostEstimate(
            flops=4 * rows * width * height, bytes_accessed=10 * rows * width, transcendentals=0
        ),
        compiler_params=granted(14),
        name="blend_rows",
    )(stream, mix, *blocks)


def slot_numbers(picks, experts):
    flat = picks.reshape(-1)
    onehot = (flat[:, None] == jnp.arange(experts, dtype=jnp.int32)[None, :]).astype(jnp.int32)
    before = jnp.cumsum(onehot, axis=0) - onehot
    return (flat, jnp.sum(before * onehot, axis=1))


def entering_state(total, me):
    size = lax.axis_size("sp")
    a, b = total[0:1], total[1:2]
    before = jnp.zeros_like(b)
    passed = jnp.ones_like(a)
    bit = 1
    while bit < size:
        other = across(jnp.concatenate([a, b], axis=0), bit)
        oa, ob = other[0:1], other[1:2]
        after = (me & bit) != 0
        before = jnp.where(after, passed * ob + before, before)
        passed = jnp.where(after, passed * oa, passed)
        b = jnp.where(after, a * ob + b, oa * b + ob)
        a = a * oa
        bit *= 2
    return before


def body(
    resid,
    recurrent_input,
    recurrent_out_gate,
    filter_weight,
    recurrence_gate_matrix,
    input_gate_matrix,
    channel_decay_raw,
    token_decay_boost,
    output_projection_weight,
    expert_norm_gain,
    routes,
    expert_pair_weight,
    gate_weight,
    up_weight,
    down_weight,
):
    tokens_here = recurrent_input.shape[0]
    tp_size, experts = lax.axis_size("tp"), lax.axis_size("sp")
    me, column = lax.axis_index("sp"), lax.axis_index("tp")
    pairs = tp_size // 2
    row, core = column // 2, column % 2
    place = jnp.stack([row, core]).astype(jnp.int32)
    rows_dev = tokens_here // tp_size
    capacity = max(2, 3 * rows_dev // experts)

    gate_own, up_own, down_all = gate_weight[0], up_weight[0], down_weight[0]
    rim = shifted(recurrent_input[tokens_here - 8 :])
    local, running, total, *halves = local_scan(
        place,
        rim,
        recurrent_input,
        filter_weight,
        recurrence_gate_matrix,
        input_gate_matrix,
        channel_decay_raw[None, :],
        token_decay_boost,
        down_all,
        pairs,
    )
    projection_far = swapped(output_projection_weight)
    gate_far, up_far = swapped(gate_own), swapped(up_own)
    down_own, down_far = [], []
    for d in range(1, pairs):
        for h in range(2):
            down_own.append(turned(halves[2 * d - 2 + h], d))
            down_far.append(swapped(down_own[-1]))
    down_whole = [down_all, swapped(down_all)]
    weights = (gate_own, up_own, gate_far, up_far, down_whole + down_own + down_far)

    own_routes = lax.dynamic_slice_in_dim(routes, column * rows_dev, rows_dev, 0)
    own_flat, own_rank = slot_numbers(own_routes, experts)
    slots = ((own_flat ^ me) * padded(capacity) + own_rank).reshape(rows_dev, 2)

    before = entering_state(total, me)
    keep, give = finish_branch(place, before, local, running, recurrent_out_gate, pairs)
    taken = swapped(give)

    def projected(d):
        near = jnp.dot(keep[d], output_projection_weight, preferred_element_type=jnp.float32)
        return near + jnp.dot(taken[d], projection_far, preferred_element_type=jnp.float32)

    pieces = [turned(projected(d).astype(jnp.bfloat16), d) for d in range(1, pairs)]
    stream, blocks = send_rows(
        resid,
        projected(0),
        pieces,
        expert_norm_gain[None, :],
        slots.T,
        experts,
        capacity,
    )
    cuts = row_cuts(experts)
    arrived = {0: blocks[0]}
    for k in range(1, experts):
        arrived[k] = across(blocks[k], k)
    own = [joined([arrived[k] for k in range(*cut)]) for cut in cuts]
    theirs = [[turned(g, d) for d in range(1, pairs)] for g in own]
    hops = range(1, pairs)
    sizes = [(cut[1] - cut[0]) * capacity for cut in cuts]
    returned = {}
    near, mid = len(cuts) // 2, 3 * len(cuts) // 4
    calls = [(0, near), (near, mid), (mid, len(cuts))]
    for first, end in calls:
        chosen = range(first, end)
        rows = [own[i] for i in chosen] + [g for i in chosen for g in theirs[i]]
        outs = [(sizes[i], jnp.float32) for i in chosen]
        outs += [(sizes[i], jnp.bfloat16) for i in chosen for _ in hops]
        results = expert_rows(place, rows, outs, weights)
        wide, narrow = results[: len(chosen)], results[len(chosen) :]
        for j, i in enumerate(chosen):
            parts = narrow[j * len(hops) : (j + 1) * len(hops)]
            backs = [turned(part, pairs - d) for part, d in zip(parts, hops)]
            sums = sum_rows(wide[j], backs, cuts[i][1] - cuts[i][0])
            for k, result in zip(range(*cuts[i]), sums):
                returned[k] = across(result, k) if k else result
    mix = mix_weights(slots, expert_pair_weight, experts * padded(capacity))
    return blend_rows(stream, mix, [returned[k] for k in range(experts)])


def joined(blocks):
    return blocks[0] if len(blocks) == 1 else jnp.concatenate(blocks, axis=0)


def row_cuts(experts):
    count = max(1, experts // 8)
    return [(k, k + count) for k in range(0, experts, count)]


def solution(mesh):
    placed = (
        P(("sp", "tp"), None),
        P("sp", "tp"),
        P("sp", "tp"),
        P(None, "tp"),
        P("tp", None, None),
        P("tp", None, None),
        P("tp"),
        P("sp", "tp"),
        P("tp", None),
        P(),
        P("sp", None),
        P(("sp", "tp"), None),
        P("sp", None, "tp"),
        P("sp", None, "tp"),
        P("sp", None, "tp"),
    )

    return jax.shard_map(
        body, mesh=mesh, in_specs=placed, out_specs=P(("sp", "tp"), None), check_vma=False
    )
```
